32 devices in a mesh: sp: 16 (over z, y, x), tp: 2 (over core).
Axes of the slice: x: 2, y: 2, z: 4, core: 2. Of those that a mesh axis runs over, the one named last changes fastest.
Arguments:
- residual: bfloat16 [4096, 2048], P(('sp', 'tp')), may hold values from -6 to 6
- queries: bfloat16 [4096, 1152], P('sp', 'tp'), may hold values from -800 to 800
- latent: bfloat16 [4096, 256], P('sp'), may hold values from -6 to 6
- rope_key: bfloat16 [4096, 32], P('sp'), may hold values from -6 to 6
- doc_ids: int32 [4096], P('sp'), may hold values from 0 to 5, never falling along the last dimension, each value on 1 to 2048 neighbouring positions
- latent_to_key: bfloat16 [256, 768], P(None, 'tp'), may hold values from -0.375 to 0.375
- latent_to_value: bfloat16 [256, 768], P(None, 'tp'), may hold values from -0.375 to 0.375
- out_proj: bfloat16 [768, 2048], replicated, may hold values from -0.21875 to 0.21875
- mix_gain: float32 [2048], replicated, may hold values from 0.1 to 1.9
- moe_gain: float32 [2048], replicated, may hold values from 0.1 to 1.9
- expert_ids: int32 [4096, 2], P(('sp', 'tp')), may hold values from 0 to 15, as said below
- route_weight: float32 [4096, 2], P(('sp', 'tp')), may hold values from 0.1 to 1
- gate_weight: bfloat16 [16, 2048, 1024], P('sp', None, 'tp'), may hold values from -0.125 to 0.125
- up_weight: bfloat16 [16, 2048, 1024], P('sp', None, 'tp'), may hold values from -0.125 to 0.125
- down_weight: bfloat16 [16, 1024, 2048], P('sp', 'tp'), may hold values from -0.1875 to 0.1875
Outputs:
- output: bfloat16 [4096, 2048], P(('sp', 'tp'))
The draws below stay inside these ranges and needn't reach their ends.
Inputs may be any that keep to these rules, and one draw needn't show every extreme that they name: `expert_ids`: each row names 2 different experts of one group of 4 consecutive numbers; in each aligned block of 128 rows (the rows of one device) no expert is named more than 32 times, and some expert exactly 32 times.
All inputs are finite; a program needn't handle non-finite values.
Results may differ from the reference program's by a relative error of at most 0.013.
Values may be sent and summed in bfloat16 or wider, within the bound.
A program may use at most 64 MiB of HBM per device.

```python
import math
import jax
import jax.numpy as jnp
import numpy as np
from jax import lax

D = 2048
HEAD_COUNT = 12
UNROTATED_DIM = 64
ROPE = 32
VALUE_ENTRIES = 64
LATENT_RANK = 256
FF = 1024
GROUPS = 4
TOP_K = 2
TOK_DEV = 256
TOKEN_COUNT = 4096
EXPERTS = 16
N_TP = 2


def rope_rows(key):
    drawn = jax.random.normal(jax.random.fold_in(key, 11), (TOKEN_COUNT, ROPE), jnp.float32)
    return jnp.clip(drawn, -6.0, 6.0)


def draw_rope_key(key, part):
    return rope_rows(key).astype(jnp.bfloat16)


def draw_queries(key, part):
    normal_part = jax.random.normal(jax.random.fold_in(key, 12), (TOKEN_COUNT, HEAD_COUNT, UNROTATED_DIM + ROPE), jnp.float32)
    normal_part = jnp.clip(normal_part, -6.0, 6.0)
    return normal_part.reshape(TOKEN_COUNT, HEAD_COUNT * (UNROTATED_DIM + ROPE)).astype(jnp.bfloat16)


def draw_expert_ids(key, part):
    row_count = TOK_DEV // N_TP
    half_rows = row_count // 2
    block_count = TOKEN_COUNT // row_count
    per_group = EXPERTS // GROUPS
    full_group = jax.random.randint(jax.random.fold_in(key, 1), (), 0, GROUPS)
    others = jax.random.randint(jax.random.fold_in(key, 2), (block_count, half_rows), 0, GROUPS - 1)
    others = others + (others >= full_group).astype(jnp.int32)
    group_ids = jnp.concatenate([jnp.full((block_count, half_rows), full_group, jnp.int32), others], axis=1)
    block_keys = jax.random.split(jax.random.fold_in(key, 3), block_count)
    group_ids = jax.vmap(lambda block_key, row_groups: jax.random.permutation(block_key, row_groups))(block_keys, group_ids)
    onehot = (group_ids[..., None] == jnp.arange(GROUPS, dtype=jnp.int32)).astype(jnp.int32)
    earlier = jnp.cumsum(onehot, axis=1) - onehot
    slot_rank = jnp.sum(earlier * onehot, axis=-1)
    offsets = jax.random.randint(jax.random.fold_in(key, 4), (block_count, GROUPS), 0, per_group)
    spacing = jax.random.randint(jax.random.fold_in(key, 5), (block_count, GROUPS), 1, per_group)
    own_offset = jnp.take_along_axis(offsets, group_ids, axis=1)
    own_spacing = jnp.take_along_axis(spacing, group_ids, axis=1)
    first_pick = (slot_rank + own_offset) % per_group
    second_pick = (slot_rank + own_offset + own_spacing) % per_group
    chosen = jnp.stack([group_ids * per_group + first_pick, group_ids * per_group + second_pick], axis=-1)
    return chosen.reshape(TOKEN_COUNT, 2).astype(jnp.int32)


def steps_of(own_key, shape, cuts, least, top_value):
    level, own = 1.0, jax.random.fold_in(own_key, 6)
    for axis_at, blocks in cuts:
        draws = jnp.exp(jax.random.uniform(jax.random.fold_in(own, axis_at), (blocks,), jnp.float32, least / len(cuts), top_value / len(cuts)))
        level = level * jnp.repeat(draws, shape[axis_at] // blocks).reshape([-1 if axis == axis_at else 1 for axis in range(len(shape))])
    return level


def profile(number_of, total, bound, slope):
    weights = [(1 << 20) // math.isqrt(rank ** slope) + 1 for rank in range(2, number_of + 1)]
    spare, counts = total - bound - (number_of - 1), [1] * (number_of - 1)
    while spare > 0:
        free = [i for i in range(number_of - 1) if counts[i] < bound]
        mass, remaining = sum([weights[i] for i in free]), spare
        for i in free:
            extra = min(bound - counts[i], max(1, remaining * weights[i] // mass), spare)
            counts[i] = counts[i] + extra
            spare = spare - extra
    return np.array([bound] + counts)


def uneven_parts(own_key, amount, total, limit, slope):
    if amount == 2:
        one = jax.random.randint(own_key, (), max(1, total - limit), min(limit, total - 1) + 1)
        return jnp.stack([one, total - one])
    tallies = jnp.asarray(profile(amount, total, limit, slope), jnp.int32)
    twos = (amount - 1) // 2
    source_of, sink = tallies[1:1 + 2 * twos:2], tallies[2:2 + 2 * twos:2]
    room = jnp.minimum(source_of - 1, limit - sink)
    moved = jax.random.randint(jax.random.fold_in(own_key, 1), (twos,), 0, 1 << 20) % (room + 1)
    tallies = tallies.at[1:1 + 2 * twos:2].set(source_of - moved).at[2:2 + 2 * twos:2].set(sink + moved)
    return tallies[jax.random.permutation(jax.random.fold_in(own_key, 2), amount)]


def bell_draw(key, extent, scale, most, cuts=(), held_as=jnp.bfloat16):
    values = scale * jax.random.normal(key, extent, jnp.float32)
    if cuts:
        values = values * steps_of(key, extent, cuts, -0.22, 0.18)
    return jnp.clip(values, -most, most).astype(held_as)


def setup_inputs(seed: int = 0) -> dict:
    arg_keys = jax.random.split(jax.random.key(seed), 16)
    return {
        "residual": bell_draw(arg_keys[0], (TOKEN_COUNT, D), 1.0, 6.0, ((0, 32),)),
        "queries": draw_queries(jax.random.fold_in(arg_keys[15], 71), 0),
        "latent": bell_draw(arg_keys[2], (TOKEN_COUNT, LATENT_RANK), 1.0, 6.0, ((0, 16),)),
        "rope_key": draw_rope_key(jax.random.fold_in(arg_keys[15], 71), 0),
        "doc_ids": jnp.searchsorted(jnp.cumsum(uneven_parts(arg_keys[4], 6, TOKEN_COUNT, TOKEN_COUNT // 2, 0)), jnp.arange(TOKEN_COUNT), side="right").astype(jnp.int32),
        "latent_to_key": bell_draw(arg_keys[5], (LATENT_RANK, HEAD_COUNT * UNROTATED_DIM), LATENT_RANK ** -0.5, 0.375, ((1, 2),)),
        "latent_to_value": bell_draw(arg_keys[6], (LATENT_RANK, HEAD_COUNT * VALUE_ENTRIES), LATENT_RANK ** -0.5, 0.375, ((1, 2),)),
        "out_proj": bell_draw(arg_keys[7], (HEAD_COUNT * VALUE_ENTRIES, D), (HEAD_COUNT * VALUE_ENTRIES) ** -0.5, 0.21875),
        "mix_gain": jnp.clip(1.0 + 0.18 * jax.random.normal(arg_keys[8], (D,), jnp.float32), 0.1, 1.9),
        "moe_gain": jnp.clip(1.0 + 0.18 * jax.random.normal(arg_keys[9], (D,), jnp.float32), 0.1, 1.9),
        "expert_ids": draw_expert_ids(jax.random.fold_in(arg_keys[15], 71), 0),
        "route_weight": jnp.clip(0.1 + 0.9 * jax.random.uniform(arg_keys[11], (TOKEN_COUNT, TOP_K), jnp.float32) ** steps_of(arg_keys[11], (TOKEN_COUNT, TOP_K), ((0, 32),), -0.2, 0.2), 0.1, 1.0),
        "gate_weight": bell_draw(arg_keys[12], (EXPERTS, D, FF), D ** -0.5, 0.125, ((0, 16), (2, 2))),
        "up_weight": bell_draw(arg_keys[13], (EXPERTS, D, FF), D ** -0.5, 0.125, ((0, 16), (2, 2))),
        "down_weight": bell_draw(arg_keys[14], (EXPERTS, FF, D), FF ** -0.5, 0.1875, ((0, 16), (1, 2))),
    }


rope_base = 10000.0
epsilon = 1e-06
query_rows = 256

def rotate(source, positions):
    half_width = source.shape[-1] // 2
    frequency = rope_base ** (-jnp.arange(half_width, dtype=jnp.float32) / half_width)
    angles = positions.astype(jnp.float32)[:, None] * frequency[None, :]
    if source.ndim == 3:
        angles = angles[:, None, :]
    cosine = jnp.cos(angles)
    sine_part = jnp.sin(angles)
    upper_half = source[..., :half_width].astype(jnp.float32)
    lower_half = source[..., half_width:].astype(jnp.float32)
    turned = jnp.concatenate([upper_half * cosine - lower_half * sine_part, lower_half * cosine + upper_half * sine_part], axis=-1)
    return turned.astype(jnp.bfloat16)

def rms_scale(source, gain):
    return source * lax.rsqrt(lax.optimization_barrier(jnp.mean(source * source, axis=-1, keepdims=True)) + epsilon) * gain

def reference(residual, queries, latent, rope_key, doc_ids, latent_to_key, latent_to_value, out_proj, mix_gain, moe_gain, expert_ids, route_weight, gate_weight, up_weight, down_weight):
    positions = jnp.arange(TOKEN_COUNT, dtype=jnp.int32)
    key_nope = jnp.dot(latent, latent_to_key, preferred_element_type=jnp.float32).astype(jnp.bfloat16)
    key_nope = key_nope.reshape(TOKEN_COUNT, HEAD_COUNT, UNROTATED_DIM).astype(jnp.float32)
    values = jnp.dot(latent, latent_to_value, preferred_element_type=jnp.float32).astype(jnp.bfloat16)
    values = values.reshape(TOKEN_COUNT, HEAD_COUNT, VALUE_ENTRIES).astype(jnp.float32)
    key_rot = rotate(rope_key, positions).astype(jnp.float32)
    shaped = queries.reshape(TOKEN_COUNT, HEAD_COUNT, UNROTATED_DIM + ROPE)
    query_nope = shaped[..., :UNROTATED_DIM]
    query_rot = rotate(shaped[..., UNROTATED_DIM:], positions)
    score_scale = (UNROTATED_DIM + ROPE) ** (-0.5)
    block_count = TOKEN_COUNT // query_rows

    def attend_rows(bundle):
        nope_block, rot_block, pos_block, doc_block = bundle
        scores = (jnp.einsum('qhd,khd->qhk', nope_block.astype(jnp.float32), key_nope) + jnp.einsum('qhr,kr->qhk', rot_block.astype(jnp.float32), key_rot)) * score_scale
        allowed = ((positions[None, :] <= pos_block[:, None]) & (doc_ids[None, :] == doc_block[:, None]))[:, None, :]
        row_max = lax.optimization_barrier(jnp.max(jnp.where(allowed, scores, -jnp.inf), axis=-1, keepdims=True))
        weights = jnp.where(allowed, jnp.exp(scores - row_max), 0.0)
        totals = lax.optimization_barrier(jnp.sum(weights, axis=-1))
        rounded = lax.optimization_barrier(weights.astype(jnp.bfloat16)).astype(jnp.float32)
        mixed = jnp.einsum('qhk,khd->qhd', rounded, values) / totals[..., None]
        return mixed.astype(jnp.bfloat16).reshape(query_rows, HEAD_COUNT * VALUE_ENTRIES)
    attended = lax.map(attend_rows, (query_nope.reshape(block_count, query_rows, HEAD_COUNT, UNROTATED_DIM), query_rot.reshape(block_count, query_rows, HEAD_COUNT, ROPE), positions.reshape(block_count, query_rows), doc_ids.reshape(block_count, query_rows)))
    attended = attended.reshape(TOKEN_COUNT, HEAD_COUNT * VALUE_ENTRIES)
    mix = jnp.dot(attended, out_proj, preferred_element_type=jnp.float32)
    branch = rms_scale(mix, mix_gain)
    middle = lax.optimization_barrier((residual.astype(jnp.float32) + branch).astype(jnp.bfloat16))
    normed = rms_scale(middle.astype(jnp.float32), moe_gain).astype(jnp.bfloat16)
    row_count = TOK_DEV // N_TP
    groups_blocks = TOKEN_COUNT // row_count
    per_group = EXPERTS // GROUPS
    capacity = row_count // per_group
    flat_ids = expert_ids.reshape(groups_blocks, row_count * TOP_K)
    onehot = (flat_ids[..., None] == jnp.arange(EXPERTS, dtype=jnp.int32)).astype(jnp.int32)
    earlier = jnp.cumsum(onehot, axis=1) - onehot
    slot_rank = lax.optimization_barrier(jnp.sum(earlier * onehot, axis=-1)).astype(jnp.int32)
    block_index = jnp.broadcast_to(jnp.arange(groups_blocks, dtype=jnp.int32)[:, None], flat_ids.shape)
    token_index = (block_index * row_count + jnp.arange(row_count * TOP_K, dtype=jnp.int32)[None, :] // TOP_K).astype(jnp.int32)
    row_table = jnp.full((EXPERTS, groups_blocks, capacity), TOKEN_COUNT, jnp.int32)
    row_table = row_table.at[flat_ids, block_index, slot_rank].set(token_index)
    weight_table = jnp.zeros((EXPERTS, groups_blocks, capacity), jnp.float32)
    weight_table = weight_table.at[flat_ids, block_index, slot_rank].set(route_weight.reshape(groups_blocks, row_count * TOP_K))
    padded = jnp.concatenate([normed, jnp.zeros((1, D), jnp.bfloat16)], axis=0)
    half_units = FF // N_TP

    def expert_step(accumulated, inputs):
        table_rows, table_weights, gate_mat, up_mat, down_mat = inputs
        picked = padded[table_rows.reshape(-1)]
        gate_out = jnp.dot(picked, gate_mat, preferred_element_type=jnp.float32)
        up_out = jnp.dot(picked, up_mat, preferred_element_type=jnp.float32)
        hidden = (jax.nn.silu(gate_out) * up_out).astype(jnp.bfloat16)
        combined = jnp.zeros((picked.shape[0], D), jnp.float32)
        for portion in range(N_TP):
            partial_value = jnp.dot(hidden[:, portion * half_units:(portion + 1) * half_units], down_mat[portion * half_units:(portion + 1) * half_units], preferred_element_type=jnp.float32)
            combined = combined + lax.optimization_barrier(partial_value.astype(jnp.bfloat16)).astype(jnp.float32)
        result = lax.optimization_barrier(combined.astype(jnp.bfloat16)).astype(jnp.float32)
        accumulated = accumulated.at[table_rows.reshape(-1)].add(result * table_weights.reshape(-1)[:, None])
        return (accumulated, None)
    accumulated, _ = lax.scan(expert_step, jnp.zeros((TOKEN_COUNT + 1, D), jnp.float32), (row_table, weight_table, gate_weight, up_weight, down_weight))
    return (middle.astype(jnp.float32) + accumulated[:TOKEN_COUNT]).astype(jnp.bfloat16)
```

```python
import functools
import math

import jax
import jax.numpy as jnp
from jax import lax
from jax.experimental import pallas as pl
from jax.experimental.pallas import tpu as pltpu
from jax.sharding import PartitionSpec as P

UNROTATED_DIM = 64
ROPE = 32
VALUE_ENTRIES = 64
GROUPS = 4
HEAD_LANES = 128
MESH = pl.DeviceIdType.MESH

rope_base = 10000.0
epsilon = 1e-06


def angles_of(positions):
    half_width = ROPE // 2
    frequency = rope_base ** (-jnp.arange(half_width, dtype=jnp.float32) / half_width)
    lane = jnp.arange(HEAD_LANES)
    turns = (lane >= UNROTATED_DIM) & (lane < UNROTATED_DIM + ROPE)
    frequency = jnp.where(turns, jnp.tile(frequency, HEAD_LANES // half_width), 0.0)
    angles = positions.astype(jnp.float32)[:, None] * frequency[None, :]
    return jnp.cos(angles), jnp.sin(angles)


def rms_scale(source, gain):
    return source * lax.rsqrt(jnp.mean(source * source, axis=-1, keepdims=True) + epsilon) * gain


def attention_kernel(
    heads, block, lo_ref, query_ref, cos_ref, sin_ref, span_ref, packed_ref, wk_ref, wv_ref, out_ref,
    turned, wide, high, total, acc,
):
    rows = query_ref.shape[0]
    width = query_ref.shape[1]
    rank = wk_ref.shape[0]
    per_head = UNROTATED_DIM + ROPE
    cosine = cos_ref[...]
    sine = sin_ref[...]
    for h in range(heads):
        first = h * per_head // 128 * 128
        last = min(-(-(h + 1) * per_head // 128) * 128, width)
        window = query_ref[:, first:last]
        shape = (last - first, HEAD_LANES)
        source = lax.broadcasted_iota(jnp.int32, shape, 0) + (first - h * per_head)
        lane = lax.broadcasted_iota(jnp.int32, shape, 1)
        half = ROPE // 2
        plain = jnp.where((source == lane) & (lane < per_head), 1.0, 0.0).astype(jnp.bfloat16)
        upper = (lane >= UNROTATED_DIM) & (lane < UNROTATED_DIM + half) & (source == lane + half)
        lower = (lane >= UNROTATED_DIM + half) & (lane < per_head) & (source == lane - half)
        crossed = (jnp.where(lower, 1.0, 0.0) - jnp.where(upper, 1.0, 0.0)).astype(jnp.bfloat16)
        straight = jnp.dot(window, plain, preferred_element_type=jnp.float32)
        swapped = jnp.dot(window, crossed, preferred_element_type=jnp.float32)
        low = h * UNROTATED_DIM // HEAD_LANES * HEAD_LANES
        pair = wk_ref[:, low : low + HEAD_LANES].astype(jnp.float32)
        if h * UNROTATED_DIM > low:
            pair = pltpu.roll(pair, HEAD_LANES - (h * UNROTATED_DIM - low), 1)
        column = lax.broadcasted_iota(jnp.int32, pair.shape, 1)
        wide[h] = jnp.where(column < UNROTATED_DIM, pair, 0.0).astype(jnp.bfloat16)
        turned[h] = (straight * cosine + swapped * sine).astype(jnp.bfloat16)
    high[...] = jnp.full(high.shape, -1e30, jnp.float32)
    total[...] = jnp.zeros(total.shape, jnp.float32)
    acc[...] = jnp.zeros(acc.shape, jnp.float32)
    span_first = span_ref[0:1, :]
    span_last = span_ref[1:2, :]
    scale = per_head ** (-0.5)

    def step(number, carry):
        base = pl.multiple_of(number * block, block)
        latent = packed_ref[pl.ds(base, block), :rank]
        extra = packed_ref[pl.ds(base, block), rank:]
        position = base + lax.broadcasted_iota(jnp.int32, (block, rows), 0)
        live = (position >= span_first) & (position <= span_last)
        values_t = lax.dot_general(
            wv_ref[...], latent, (((0,), (1,)), ((), ())), preferred_element_type=jnp.float32
        ).astype(jnp.bfloat16)
        for h in range(heads):
            keys = jnp.dot(
                latent, wide[h],
                preferred_element_type=jnp.float32,
            ).astype(jnp.bfloat16) + extra
            scores = lax.dot_general(
                keys, turned[h], (((1,), (1,)), ((), ())), preferred_element_type=jnp.float32
            ) * scale
            scores = jnp.where(live, scores, -1e30)
            old = high[h : h + 1, :]
            new = jnp.maximum(old, jnp.max(scores, axis=0, keepdims=True))
            weights = jnp.where(live, jnp.exp(scores - new), 0.0)
            factor = jnp.exp(old - new)
            high[h : h + 1, :] = new
            total[h : h + 1, :] = total[h : h + 1, :] * factor + jnp.sum(
                weights, axis=0, keepdims=True
            )
            acc[h] = acc[h] * factor + jnp.dot(
                values_t[h * VALUE_ENTRIES : (h + 1) * VALUE_ENTRIES],
                weights.astype(jnp.bfloat16),
                preferred_element_type=jnp.float32,
            )
        return carry

    lax.fori_loop(lo_ref[0], lo_ref[1], step, 0)
    for h in range(heads):
        out_ref[h * VALUE_ENTRIES : (h + 1) * VALUE_ENTRIES, :] = (
            acc[h] / total[h : h + 1, :]
        ).astype(jnp.bfloat16)


def attend(queries, packed, doc_ids, latent_to_key, latent_to_value, positions, cosine, sine):
    rows = queries.shape[0]
    heads = queries.shape[1] // (UNROTATED_DIM + ROPE)
    rank = latent_to_key.shape[0]
    count = packed.shape[0]
    place = jnp.arange(count, dtype=jnp.int32)
    docs = packed[:, rank + UNROTATED_DIM + ROPE].astype(jnp.int32)
    docs = jnp.where(place < positions[0] - count // 2, -1, docs)
    docs = jnp.where(place > positions[-1], jnp.iinfo(jnp.int32).max, docs)
    starts = jnp.sum((docs[:, None] < doc_ids[None, :]).astype(jnp.int32), axis=0)
    block = math.gcd(count, 256)
    bounds = jnp.stack([starts[0] // block, positions[-1] // block + 1]).astype(jnp.int32)
    span = jnp.stack([starts, positions])
    vmem = pl.BlockSpec(memory_space=pltpu.VMEM)
    out = pl.pallas_call(
        functools.partial(attention_kernel, heads, block),
        out_shape=jax.ShapeDtypeStruct((heads * VALUE_ENTRIES, rows), jnp.bfloat16),
        in_specs=[pl.BlockSpec(memory_space=pltpu.SMEM)] + [vmem] * 7,
        out_specs=vmem,
        scratch_shapes=[
            pltpu.VMEM((heads, rows, HEAD_LANES), jnp.bfloat16),
            pltpu.VMEM((heads, rank, HEAD_LANES), jnp.bfloat16),
            pltpu.VMEM((heads, rows), jnp.float32),
            pltpu.VMEM((heads, rows), jnp.float32),
            pltpu.VMEM((heads, VALUE_ENTRIES, rows), jnp.float32),
        ],
        compiler_params=pltpu.CompilerParams(vmem_limit_bytes=40 * 1024 * 1024),
        name="attend",
    )(bounds, queries, cosine, sine, span, packed, latent_to_key, latent_to_value)
    return out.T


def greet(groups, plane):
    index, core = lax.axis_index("sp"), lax.axis_index("tp")
    level, place = index // plane, lax.rem(index, plane)
    barrier = pltpu.get_barrier_semaphore()
    peers = [(lax.rem(level + d, groups) * plane + place, core) for d in range(1, groups)]
    peers += [(level * plane + lax.rem(place + d, plane), core) for d in range(1, plane)]
    peers += [(index, 1 - core)]
    for peer in peers:
        pl.semaphore_signal(barrier, inc=1, device_id=peer, device_id_type=MESH)
    pl.semaphore_wait(barrier, len(peers))
    return index, core, level, place


def remote(source, target, send_sem, recv_sem, peer):
    return pltpu.make_async_remote_copy(
        src_ref=source, dst_ref=target, send_sem=send_sem, recv_sem=recv_sem,
        device_id=peer, device_id_type=MESH,
    )


def level_order(groups):
    return sorted(range(groups), key=lambda d: min(d, groups - d))


def nearest(level, groups, at):
    picked = 0
    for l in range(groups):
        choice = sorted(range(groups), key=lambda s: (abs(s - l), s))[at]
        picked = picked + jnp.where(level == l, choice, 0)
    return picked


def expert_kernel(
    groups, plane, capacity, rows_ref, meta_ref, gate_ref, up_ref, down_ref, out_ref,
    gate, up, down, metas, landed, spread, arrived, hidden, partial, passed, mixed, back, merged,
    w_sem, m_send, m_recv, z_send, z_recv, p_send, p_recv, own_sem, t_send, t_recv,
    x_send, x_recv, b_send, b_recv, keep_sem, r_send, r_recv,
):
    weights = [
        pltpu.make_async_copy(source, target, w_sem.at[i])
        for i, (source, target) in enumerate([(gate_ref, gate), (up_ref, up), (down_ref, down)])
    ]
    for copy in weights:
        copy.start()
    index, core, level, place = greet(groups, plane)
    started = []
    slots = plane * capacity
    group_rows = rows_ref.shape[1]
    width = rows_ref.shape[2]
    source_of = [nearest(level, groups, k) for k in range(groups)]

    def begin(copy):
        copy.start()
        started.append(copy)

    for k in range(1, groups):
        other = source_of[k]
        peer = (other * plane + place, core)
        begin(remote(meta_ref.at[other], metas.at[level], m_send.at[k], m_recv.at[level], peer))
        begin(remote(rows_ref.at[other], landed.at[level], z_send.at[k], z_recv.at[level], peer))
    metas[level] = meta_ref[level]

    def send_out(k):
        source = source_of[k]
        if k == 0:
            rows = rows_ref[level]
        else:
            peer = (source * plane + place, core)
            remote(meta_ref.at[source], metas.at[source], m_send.at[k], m_recv.at[source], peer).wait_recv()
            remote(rows_ref.at[source], landed.at[source], z_send.at[k], z_recv.at[source], peer).wait_recv()
            rows = landed[source]
        info = metas[source][:, :group_rows].astype(jnp.float32)
        slot = lax.broadcasted_iota(jnp.int32, (slots, group_rows), 0).astype(jnp.float32)
        chooser = jnp.where((slot == info[0:1]) | (slot == info[1:2]), 1.0, 0.0)
        picked = jnp.dot(chooser.astype(jnp.bfloat16), rows, preferred_element_type=jnp.float32)
        for e in range(plane):
            spread[k, e] = picked[e * capacity : (e + 1) * capacity].astype(jnp.bfloat16)
        for far in range(plane - 1, 0, -1):
            to = lax.rem(place + far, plane)
            begin(remote(
                spread.at[k, to], arrived.at[k, core, place],
                p_send.at[k * plane + far], p_recv.at[k * plane + place],
                (level * plane + to, core),
            ))
        pltpu.make_async_copy(
            spread.at[k, place], arrived.at[k, core, place], own_sem.at[k]
        ).start()

    def hand_over(k):
        for far in range(plane):
            origin = lax.rem(place + plane - far, plane)
            if far:
                remote(
                    spread.at[k, origin], arrived.at[k, core, origin],
                    p_send.at[k * plane + far], p_recv.at[k * plane + origin],
                    (level * plane + origin, core),
                ).wait_recv()
            else:
                pltpu.make_async_copy(
                    spread.at[k, place], arrived.at[k, core, place], own_sem.at[k]
                ).wait()
            begin(remote(
                arrived.at[k, core, origin], arrived.at[k, core, origin],
                t_send.at[k * plane + far], t_recv.at[k * plane + origin], (index, 1 - core),
            ))

    def experts(k):
        for origin in range(plane):
            remote(
                arrived.at[k, 1 - core, origin], arrived.at[k, 1 - core, origin],
                t_send.at[k * plane], t_recv.at[k * plane + origin], (index, 1 - core),
            ).wait_recv()
        units = gate.shape[1]
        unit_tile = math.gcd(units, 256)
        tile = math.gcd(width, 256)

        def hide(j, carry):
            columns = pl.ds(pl.multiple_of(j * unit_tile, unit_tile), unit_tile)
            rows = arrived[k].reshape(2 * slots, width)
            gated = jnp.dot(rows, gate[:, columns], preferred_element_type=jnp.float32)
            raised = jnp.dot(rows, up[:, columns], preferred_element_type=jnp.float32)
            hidden[:, columns] = (gated / (1.0 + jnp.exp(-gated)) * raised).astype(jnp.bfloat16)
            return carry

        lax.fori_loop(0, units // unit_tile, hide, 0)

        def lower(j, carry):
            columns = pl.ds(pl.multiple_of(j * tile, tile), tile)
            piece = jnp.dot(hidden[...], down[:, columns], preferred_element_type=jnp.float32)
            partial[k, :, :, :, columns] = piece.reshape(2, plane, capacity, tile).astype(jnp.bfloat16)
            return carry

        lax.fori_loop(0, width // tile, lower, 0)
        begin(remote(
            partial.at[k, 1 - core], passed.at[k], x_send.at[k], x_recv.at[k], (index, 1 - core)
        ))

    def send_back(k):
        remote(
            partial.at[k, core], passed.at[k], x_send.at[k], x_recv.at[k], (index, 1 - core)
        ).wait_recv()
        for e in range(plane):
            mixed[k, e] = (
                partial[k, core, e].astype(jnp.float32) + passed[k, e].astype(jnp.float32)
            ).astype(jnp.bfloat16)
        for far in range(plane - 1, 0, -1):
            to = lax.rem(place + far, plane)
            begin(remote(
                mixed.at[k, to], back.at[k, place],
                b_send.at[k * plane + far], b_recv.at[k * plane + place],
                (level * plane + to, core),
            ))
        pltpu.make_async_copy(mixed.at[k, place], back.at[k, place], keep_sem.at[k]).start()

    def combine(k):
        source = source_of[k]
        for far in range(1, plane):
            origin = lax.rem(place + plane - far, plane)
            remote(
                mixed.at[k, origin], back.at[k, origin],
                b_send.at[k * plane + far], b_recv.at[k * plane + origin],
                (level * plane + origin, core),
            ).wait_recv()
        pltpu.make_async_copy(mixed.at[k, place], back.at[k, place], keep_sem.at[k]).wait()
        info = metas[source][:, :group_rows].astype(jnp.float32)
        slot = lax.broadcasted_iota(jnp.int32, (slots, group_rows), 0).astype(jnp.float32)
        hit_first, hit_second = slot == info[0:1], slot == info[1:2]
        returned = back[k].reshape(slots, width)
        result = 0.0
        for term in range(2):
            share = jnp.where(hit_first, info[2 + term : 3 + term], 0.0) + jnp.where(
                hit_second, info[4 + term : 5 + term], 0.0
            )
            result = result + lax.dot_general(
                share.astype(jnp.bfloat16), returned, (((0,), (0,)), ((), ())),
                preferred_element_type=jnp.float32,
            )
        if k == 0:
            out_ref[level] = result.astype(jnp.bfloat16)
        else:
            merged[k] = result.astype(jnp.bfloat16)
            begin(remote(
                merged.at[k], out_ref.at[level], r_send.at[k], r_recv.at[level],
                (source * plane + place, core),
            ))

    send_out(0)
    send_out(1)
    hand_over(0)
    for copy in weights:
        copy.wait()
    experts(0)
    send_back(0)
    for k in range(1, groups):
        if k + 1 < groups:
            send_out(k + 1)
        hand_over(k)
        experts(k)
        if k > 1:
            combine(k - 1)
        send_back(k)
    combine(groups - 1)
    combine(0)
    for k in range(1, groups):
        other = source_of[k]
        remote(
            merged.at[k], out_ref.at[other], r_send.at[k], r_recv.at[other],
            (other * plane + place, core),
        ).wait_recv()
    for copy in started:
        copy.wait_send()


def run_experts(rows, meta, gate, up, down, plane, capacity):
    groups, group_rows, width = rows.shape
    units = gate.shape[1]
    vmem = pl.BlockSpec(memory_space=pltpu.VMEM)
    hbm = pl.BlockSpec(memory_space=pl.ANY)
    dma = pltpu.SemaphoreType.DMA
    few, many = dma((groups,)), dma((groups * plane,))

    def held(*shape):
        return pltpu.VMEM(shape, jnp.bfloat16)

    block = held(groups, plane, capacity, width)
    double = held(groups, 2, plane, capacity, width)
    return pl.pallas_call(
        functools.partial(expert_kernel, groups, plane, capacity),
        out_shape=jax.ShapeDtypeStruct((groups, group_rows, width), jnp.bfloat16),
        in_specs=[vmem, vmem, hbm, hbm, hbm],
        out_specs=vmem,
        scratch_shapes=[
            held(*gate.shape), held(*up.shape), held(*down.shape), held(*meta.shape),
            held(groups, group_rows, width), block, double,
            held(2 * plane * capacity, units), double, block, block, block,
            held(groups, group_rows, width),
            dma((3,)), few, few, few, few, many, many, few, many, many,
            few, few, many, many, few, few, few,
        ],
        compiler_params=pltpu.CompilerParams(
            collective_id=1, has_side_effects=True, vmem_limit_bytes=48 * 1024 * 1024
        ),
        name="run_experts",
    )(rows, meta, gate, up, down)


def spread_kernel(
    groups, plane, own_ref, out_ref, z_send, z_recv, p_send, p_recv, t_send, t_recv
):
    index, core, level, place = greet(groups, plane)
    reach = groups // 2
    rows = own_ref.shape[0]
    half = rows // 2
    mine = pl.ds(pl.multiple_of(core * half, half), half)
    other = pl.ds(pl.multiple_of((1 - core) * half, half), half)

    def z_copy(d):
        return remote(
            own_ref.at[mine], out_ref.at[index, mine], z_send.at[d], z_recv.at[d],
            (lax.rem(level + d, groups) * plane + place, core),
        )

    def z_arrival(d):
        block = lax.rem(level + groups - d, groups) * plane + place
        return remote(
            own_ref.at[mine], out_ref.at[block, mine], z_send.at[d], z_recv.at[d],
            (block, core),
        )

    def p_copy(d, far):
        block = lax.rem(level + groups - d, groups) * plane + place
        source = own_ref.at[mine] if d == 0 else out_ref.at[block, mine]
        return remote(
            source, out_ref.at[block, mine], p_send.at[d * plane + far],
            p_recv.at[d * plane + far],
            (level * plane + lax.rem(place + far, plane), core),
        )

    def p_arrival(d, far):
        origin = lax.rem(place + plane - far, plane)
        block = lax.rem(level + groups - d, groups) * plane + origin
        return remote(
            own_ref.at[mine], out_ref.at[block, mine], p_send.at[d * plane + far],
            p_recv.at[d * plane + far], (level * plane + origin, core),
        )

    def t_copy(d, far, part):
        origin = lax.rem(place + plane - far, plane)
        block = lax.rem(level + groups - d, groups) * plane + origin
        return remote(
            out_ref.at[block, part], out_ref.at[block, part], t_send.at[d * plane + far],
            t_recv.at[d * plane + far], (index, 1 - core),
        )

    def wanted(d, far, sender):
        ahead = lax.rem(place + far, plane) > place if sender else place >= far
        live = level >= d
        if d == 0:
            return live & ahead
        if d == reach:
            return live & jnp.logical_not(ahead)
        return live

    for d in range(reach, 0, -1):
        pl.when(level + d < groups)(lambda d=d: z_copy(d).start())
    for far in range(1, plane):
        pl.when(wanted(0, far, True))(lambda far=far: p_copy(0, far).start())
    out_ref[index] = own_ref[...]
    for d in range(1, reach + 1):

        def arrived(d=d):
            z_arrival(d).wait_recv()
            t_copy(d, 0, mine).start()

        pl.when(level >= d)(arrived)
        for far in range(1, plane):
            pl.when(wanted(d, far, True))(lambda d=d, far=far: p_copy(d, far).start())
    for d in range(reach + 1):
        for far in range(1, plane):

            def passed_on(d=d, far=far):
                p_arrival(d, far).wait_recv()
                t_copy(d, far, mine).start()

            pl.when(wanted(d, far, False))(passed_on)
    for d in range(reach + 1):
        for far in range(0 if d else 1, plane):

            def from_partner(d=d, far=far):
                t_copy(d, far, other).wait_recv()
                t_copy(d, far, mine).wait_send()

            pl.when((level >= d) if far == 0 else wanted(d, far, False))(from_partner)
            if far:
                pl.when(wanted(d, far, True))(lambda d=d, far=far: p_copy(d, far).wait_send())
    for d in range(1, reach + 1):
        pl.when(level + d < groups)(lambda d=d: z_copy(d).wait_send())


def spread_blocks(own, count):
    rows, lanes = own.shape
    plane = count // GROUPS
    vmem = pl.BlockSpec(memory_space=pltpu.VMEM)
    few = pltpu.SemaphoreType.DMA((GROUPS,))
    many = pltpu.SemaphoreType.DMA((GROUPS * plane,))
    return pl.pallas_call(
        functools.partial(spread_kernel, GROUPS, plane),
        out_shape=jax.ShapeDtypeStruct((count, rows, lanes), jnp.bfloat16),
        in_specs=[vmem],
        out_specs=vmem,
        scratch_shapes=[few, few, many, many, many, many],
        compiler_params=pltpu.CompilerParams(
            collective_id=3, has_side_effects=True, vmem_limit_bytes=40 * 1024 * 1024
        ),
        name="spread_blocks",
    )(own).reshape(count * rows, lanes)


def local(
    residual,
    queries,
    latent,
    rope_key,
    doc_ids,
    latent_to_key,
    latent_to_value,
    out_proj,
    mix_gain,
    moe_gain,
    expert_ids,
    route_weight,
    gate_weight,
    up_weight,
    down_weight,
):
    local_rows = queries.shape[0]
    positions = lax.axis_index("sp") * local_rows + jnp.arange(local_rows, dtype=jnp.int32)
    cosine, sine = angles_of(positions)
    half = ROPE // 2
    after = HEAD_LANES - UNROTATED_DIM - ROPE
    key = rope_key.astype(jnp.float32)
    crossed = jnp.concatenate([-key[:, half:], key[:, :half]], axis=1)
    around = ((0, 0), (UNROTATED_DIM, after))
    extra = jnp.pad(key, around) * cosine + jnp.pad(crossed, around) * sine
    lane = jnp.arange(HEAD_LANES)[None, :]
    extra = jnp.where(
        lane == UNROTATED_DIM + ROPE, doc_ids.astype(jnp.float32)[:, None], extra
    ).astype(jnp.bfloat16)
    own = jnp.concatenate([latent, extra], axis=1)
    packed = spread_blocks(own, lax.axis_size("sp"))
    attended = attend(
        queries, packed, doc_ids, latent_to_key, latent_to_value, positions, cosine, sine
    )
    gathered = lax.all_to_all(attended, "tp", split_axis=0, concat_axis=1, tiled=True)
    mix = jnp.dot(gathered, out_proj, preferred_element_type=jnp.float32)
    branch = rms_scale(mix, mix_gain)
    middle = lax.optimization_barrier((residual.astype(jnp.float32) + branch).astype(jnp.bfloat16))
    normed = rms_scale(middle.astype(jnp.float32), moe_gain).astype(jnp.bfloat16)
    row_count = normed.shape[0]
    width = normed.shape[1]
    top_count = expert_ids.shape[1]
    expert_count = lax.axis_size("sp")
    capacity = row_count // (expert_count // GROUPS)
    plane = expert_count // GROUPS
    group_rows = capacity * plane // top_count
    group_of = expert_ids[:, 0] // plane
    bins = jnp.arange(expert_count + GROUPS, dtype=jnp.int32)[None, :]
    group_bin = group_of[:, None] + expert_count
    named = jnp.any(expert_ids[:, :, None] == bins[None], axis=1) | (group_bin == bins)
    before = jnp.arange(row_count)[:, None] > jnp.arange(row_count)[None, :]
    earlier = jnp.dot(
        before.astype(jnp.bfloat16), named.astype(jnp.bfloat16), preferred_element_type=jnp.float32
    ).astype(jnp.int32)
    slot_rank = jnp.sum(jnp.where(expert_ids[:, :, None] == bins[None], earlier[:, None], 0), axis=2)
    group_rank = jnp.sum(jnp.where(group_bin == bins, earlier, 0), axis=1)
    slots = lax.rem(expert_ids, plane) * capacity + slot_rank
    member = (group_of * group_rows + group_rank)[:, None]
    chooser = (member == jnp.arange(GROUPS * group_rows, dtype=jnp.int32)[None, :]).astype(
        jnp.bfloat16
    )
    coarse = route_weight.astype(jnp.bfloat16)
    fine = (route_weight - coarse.astype(jnp.float32)).astype(jnp.bfloat16)
    fields = jnp.concatenate(
        [
            (slots + 1).astype(jnp.bfloat16),
            jnp.stack([coarse[:, 0], fine[:, 0], coarse[:, 1], fine[:, 1]], axis=1),
        ],
        axis=1,
    )
    fields = jnp.pad(fields, ((0, 0), (0, 16 - fields.shape[1])))
    meta = lax.dot_general(
        fields, chooser, (((0,), (0,)), ((), ())), preferred_element_type=jnp.float32
    )
    meta = meta - (jnp.arange(16) < top_count)[:, None].astype(jnp.float32)
    meta = meta.astype(jnp.bfloat16).reshape(16, GROUPS, group_rows).transpose(1, 0, 2)
    meta = jnp.pad(meta, ((0, 0), (0, 0), (0, -group_rows % 128)))
    grouped = lax.dot_general(
        chooser, normed, (((0,), (0,)), ((), ())), preferred_element_type=jnp.float32
    ).astype(jnp.bfloat16)
    returned = run_experts(
        grouped.reshape(GROUPS, group_rows, width), meta, gate_weight[0], up_weight[0],
        down_weight[0], plane, capacity,
    )
    expert_mix = jnp.dot(
        chooser, returned.reshape(-1, width), preferred_element_type=jnp.float32
    )
    return (middle.astype(jnp.float32) + expert_mix).astype(jnp.bfloat16)


def solution(mesh):
    in_specs = (
        P(("sp", "tp"), None),
        P("sp", "tp"),
        P("sp", None),
        P("sp", None),
        P("sp"),
        P(None, "tp"),
        P(None, "tp"),
        P(),
        P(),
        P(),
        P(("sp", "tp"), None),
        P(("sp", "tp"), None),
        P("sp", None, "tp"),
        P("sp", None, "tp"),
        P("sp", "tp", None),
    )
    out_specs = P(("sp", "tp"), None)
    return jax.shard_map(local, mesh=mesh, in_specs=in_specs, out_specs=out_specs, check_vma=False)
```

```python
import functools
import math

import jax
import jax.numpy as jnp
from jax import lax
from jax.experimental import pallas as pl
from jax.experimental.pallas import tpu as pltpu
from jax.sharding import PartitionSpec as P

UNROTATED_DIM = 64
ROPE = 32
VALUE_ENTRIES = 64
GROUPS = 4
HEAD_LANES = 128
MESH = pl.DeviceIdType.MESH

rope_base = 10000.0
epsilon = 1e-06


def angles_of(positions):
    half_width = ROPE // 2
    frequency = rope_base ** (-jnp.arange(half_width, dtype=jnp.float32) / half_width)
    angles = frequency[:, None] * positions.astype(jnp.float32)[None, :]
    return jnp.cos(angles), jnp.sin(angles)


def rms_scale(source, gain):
    return source * lax.rsqrt(jnp.mean(source * source, axis=-1, keepdims=True) + epsilon) * gain


def turn(pair, cosine, sine):
    half = ROPE // 2
    upper, lower = pair[:half].astype(jnp.float32), pair[half:].astype(jnp.float32)
    return jnp.concatenate(
        [upper * cosine - lower * sine, lower * cosine + upper * sine], axis=0
    ).astype(jnp.bfloat16)


def greet(groups, plane, meanwhile=None):
    index, core = lax.axis_index("sp"), lax.axis_index("tp")
    level, place = index // plane, lax.rem(index, plane)
    barrier = pltpu.get_barrier_semaphore()
    peers = [(lax.rem(level + d, groups) * plane + place, core) for d in range(1, groups)]
    peers += [(level * plane + lax.rem(place + d, plane), core) for d in range(1, plane)]
    peers += [(index, 1 - core)]
    for peer in peers:
        pl.semaphore_signal(barrier, inc=1, device_id=peer, device_id_type=MESH)
    if meanwhile is not None:
        meanwhile(index, core)
    pl.semaphore_wait(barrier, len(peers))
    return index, core, level, place


def remote(source, target, send_sem, recv_sem, peer):
    return pltpu.make_async_remote_copy(
        src_ref=source, dst_ref=target, send_sem=send_sem, recv_sem=recv_sem,
        device_id=peer, device_id_type=MESH,
    )


def level_order(groups):
    return sorted(range(groups), key=lambda d: min(d, groups - d))


def nearest(level, groups, at):
    picked = 0
    for l in range(groups):
        choice = sorted(range(groups), key=lambda s: (abs(s - l), s))[at]
        picked = picked + jnp.where(level == l, choice, 0)
    return picked


def expert_kernel(
    groups, plane, capacity, rows_ref, meta_ref, gate_ref, up_ref, down_ref, out_ref,
    gate, up, down, metas, landed, spread, arrived, hidden, partial, passed, mixed, back, merged,
    w_sem, m_send, m_recv, z_send, z_recv, p_send, p_recv, own_sem, t_send, t_recv,
    x_send, x_recv, b_send, b_recv, keep_sem, r_send, r_recv,
):
    weights = [
        pltpu.make_async_copy(source, target, w_sem.at[i])
        for i, (source, target) in enumerate([(gate_ref, gate), (up_ref, up), (down_ref, down)])
    ]
    for copy in weights:
        copy.start()
    index, core, level, place = greet(groups, plane)
    started = []
    slots = plane * capacity
    group_rows = rows_ref.shape[1]
    width = rows_ref.shape[2]
    source_of = [nearest(level, groups, k) for k in range(groups)]

    def begin(copy):
        copy.start()
        started.append(copy)

    for k in range(1, groups):
        other = source_of[k]
        peer = (other * plane + place, core)
        begin(remote(meta_ref.at[other], metas.at[level], m_send.at[k], m_recv.at[level], peer))
        begin(remote(rows_ref.at[other], landed.at[level], z_send.at[k], z_recv.at[level], peer))
    metas[level] = meta_ref[level]

    def send_out(k):
        source = source_of[k]
        if k == 0:
            rows = rows_ref[level]
        else:
            peer = (source * plane + place, core)
            remote(meta_ref.at[source], metas.at[source], m_send.at[k], m_recv.at[source], peer).wait_recv()
            remote(rows_ref.at[source], landed.at[source], z_send.at[k], z_recv.at[source], peer).wait_recv()
            rows = landed[source]
        info = metas[source][:, :group_rows].astype(jnp.float32)
        slot = lax.broadcasted_iota(jnp.int32, (slots, group_rows), 0).astype(jnp.float32)
        chooser = jnp.where((slot == info[0:1]) | (slot == info[1:2]), 1.0, 0.0)
        picked = jnp.dot(chooser.astype(jnp.bfloat16), rows, preferred_element_type=jnp.float32)
        for e in range(plane):
            spread[k, e] = picked[e * capacity : (e + 1) * capacity].astype(jnp.bfloat16)
        for far in range(plane - 1, 0, -1):
            to = lax.rem(place + far, plane)
            begin(remote(
                spread.at[k, to], arrived.at[k, core, place],
                p_send.at[k * plane + far], p_recv.at[k * plane + place],
                (level * plane + to, core),
            ))
        pltpu.make_async_copy(
            spread.at[k, place], arrived.at[k, core, place], own_sem.at[k]
        ).start()

    def hand_over(k):
        for far in range(plane):
            origin = lax.rem(place + plane - far, plane)
            if far:
                remote(
                    spread.at[k, origin], arrived.at[k, core, origin],
                    p_send.at[k * plane + far], p_recv.at[k * plane + origin],
                    (level * plane + origin, core),
                ).wait_recv()
            else:
                pltpu.make_async_copy(
                    spread.at[k, place], arrived.at[k, core, place], own_sem.at[k]
                ).wait()
            begin(remote(
                arrived.at[k, core, origin], arrived.at[k, core, origin],
                t_send.at[k * plane + far], t_recv.at[k * plane + origin], (index, 1 - core),
            ))

    def experts(k):
        for origin in range(plane):
            remote(
                arrived.at[k, 1 - core, origin], arrived.at[k, 1 - core, origin],
                t_send.at[k * plane], t_recv.at[k * plane + origin], (index, 1 - core),
            ).wait_recv()
        units = gate.shape[1]
        unit_tile = math.gcd(units, 256)
        tile = math.gcd(width, 256)

        def hide(j, carry):
            columns = pl.ds(pl.multiple_of(j * unit_tile, unit_tile), unit_tile)
            rows = arrived[k].reshape(2 * slots, width)
            gated = jnp.dot(rows, gate[:, columns], preferred_element_type=jnp.float32)
            raised = jnp.dot(rows, up[:, columns], preferred_element_type=jnp.float32)
            hidden[:, columns] = (gated / (1.0 + jnp.exp(-gated)) * raised).astype(jnp.bfloat16)
            return carry

        lax.fori_loop(0, units // unit_tile, hide, 0)

        def lower(j, carry):
            columns = pl.ds(pl.multiple_of(j * tile, tile), tile)
            piece = jnp.dot(hidden[...], down[:, columns], preferred_element_type=jnp.float32)
            partial[k, :, :, :, columns] = piece.reshape(2, plane, capacity, tile).astype(jnp.bfloat16)
            return carry

        lax.fori_loop(0, width // tile, lower, 0)
        begin(remote(
            partial.at[k, 1 - core], passed.at[k], x_send.at[k], x_recv.at[k], (index, 1 - core)
        ))

    def send_back(k):
        remote(
            partial.at[k, core], passed.at[k], x_send.at[k], x_recv.at[k], (index, 1 - core)
        ).wait_recv()
        for e in range(plane):
            mixed[k, e] = (
                partial[k, core, e].astype(jnp.float32) + passed[k, e].astype(jnp.float32)
            ).astype(jnp.bfloat16)
        for far in range(plane - 1, 0, -1):
            to = lax.rem(place + far, plane)
            begin(remote(
                mixed.at[k, to], back.at[k, place],
                b_send.at[k * plane + far], b_recv.at[k * plane + place],
                (level * plane + to, core),
            ))
        pltpu.make_async_copy(mixed.at[k, place], back.at[k, place], keep_sem.at[k]).start()

    def combine(k):
        source = source_of[k]
        for far in range(1, plane):
            origin = lax.rem(place + plane - far, plane)
            remote(
                mixed.at[k, origin], back.at[k, origin],
                b_send.at[k * plane + far], b_recv.at[k * plane + origin],
                (level * plane + origin, core),
            ).wait_recv()
        pltpu.make_async_copy(mixed.at[k, place], back.at[k, place], keep_sem.at[k]).wait()
        info = metas[source][:, :group_rows].astype(jnp.float32)
        slot = lax.broadcasted_iota(jnp.int32, (slots, group_rows), 0).astype(jnp.float32)
        hit_first, hit_second = slot == info[0:1], slot == info[1:2]
        returned = back[k].reshape(slots, width)
        result = 0.0
        for term in range(2):
            share = jnp.where(hit_first, info[2 + term : 3 + term], 0.0) + jnp.where(
                hit_second, info[4 + term : 5 + term], 0.0
            )
            result = result + lax.dot_general(
                share.astype(jnp.bfloat16), returned, (((0,), (0,)), ((), ())),
                preferred_element_type=jnp.float32,
            )
        if k == 0:
            out_ref[level] = result.astype(jnp.bfloat16)
        else:
            merged[k] = result.astype(jnp.bfloat16)
            begin(remote(
                merged.at[k], out_ref.at[level], r_send.at[k], r_recv.at[level],
                (source * plane + place, core),
            ))

    send_out(0)
    send_out(1)
    hand_over(0)
    for copy in weights:
        copy.wait()
    experts(0)
    send_back(0)
    for k in range(1, groups):
        if k + 1 < groups:
            send_out(k + 1)
        hand_over(k)
        experts(k)
        if k > 1:
            combine(k - 1)
        send_back(k)
    combine(groups - 1)
    combine(0)
    for k in range(1, groups):
        other = source_of[k]
        remote(
            merged.at[k], out_ref.at[other], r_send.at[k], r_recv.at[other],
            (other * plane + place, core),
        ).wait_recv()
    for copy in started:
        copy.wait_send()


def run_experts(rows, meta, gate, up, down, plane, capacity):
    groups, group_rows, width = rows.shape
    units = gate.shape[1]
    vmem = pl.BlockSpec(memory_space=pltpu.VMEM)
    hbm = pl.BlockSpec(memory_space=pl.ANY)
    dma = pltpu.SemaphoreType.DMA
    few, many = dma((groups,)), dma((groups * plane,))

    def held(*shape):
        return pltpu.VMEM(shape, jnp.bfloat16)

    block = held(groups, plane, capacity, width)
    double = held(groups, 2, plane, capacity, width)
    return pl.pallas_call(
        functools.partial(expert_kernel, groups, plane, capacity),
        out_shape=jax.ShapeDtypeStruct((groups, group_rows, width), jnp.bfloat16),
        in_specs=[vmem, vmem, hbm, hbm, hbm],
        out_specs=vmem,
        scratch_shapes=[
            held(*gate.shape), held(*up.shape), held(*down.shape), held(*meta.shape),
            held(groups, group_rows, width), block, double,
            held(2 * plane * capacity, units), double, block, block, block,
            held(groups, group_rows, width),
            dma((3,)), few, few, few, few, many, many, few, many, many,
            few, few, many, many, few, few, few,
        ],
        compiler_params=pltpu.CompilerParams(
            collective_id=1, has_side_effects=True, vmem_limit_bytes=48 * 1024 * 1024
        ),
        name="run_experts",
    )(rows, meta, gate, up, down)


def attend_kernel(
    groups, plane, heads,
    query_hbm, latent_hbm, rope_hbm, wk_hbm, wv_hbm, proj_hbm, residual_hbm,
    cos_ref, sin_ref, docs_ref, member_ref, mix_gain_ref, moe_gain_ref,
    middle_ref, grouped_ref,
    query, latent, rope, wk, wv, proj, residual,
    packs, turned, wv_turned, high, total, acc, halves, full, mix, normed,
    load_sem, z_send, z_recv, p_send, p_recv, t_send, t_recv, x_send, x_recv,
):
    loads = [
        pltpu.make_async_copy(source, target, load_sem.at[i])
        for i, (source, target) in enumerate([
            (latent_hbm, latent), (rope_hbm, rope), (query_hbm, query), (wk_hbm, wk),
            (wv_hbm, wv), (residual_hbm, residual), (proj_hbm, proj),
        ])
    ]
    for copy in loads:
        copy.start()
    rows = latent.shape[0]
    half = rows // 2
    per_head = UNROTATED_DIM + ROPE
    cosine, sine = cos_ref[...], sin_ref[...]
    docs = docs_ref[...]

    def pack(index, core):
        loads[0].wait()
        loads[1].wait()
        key = turn(rope[...], cosine, sine)
        for part in range(2):
            span = slice(part * half, (part + 1) * half)
            packs[index, part, :half, :] = latent[span, :]
            line = lax.broadcasted_iota(jnp.int32, (ROPE, half), 0)
            ids = jnp.where(line == 0, jnp.broadcast_to(docs[:, span], (ROPE, half)), 0.0)
            packs[index, part, half:, :half] = key[:, span]
            packs[index, part, half:, half : 2 * half] = ids.astype(jnp.bfloat16)

    index, core, level, place = greet(groups, plane, pack)
    reach = groups // 2

    def z_copy(d):
        return remote(
            packs.at[index, core], packs.at[index, core], z_send.at[d], z_recv.at[d],
            (lax.rem(level + d, groups) * plane + place, core),
        )

    def z_arrival(d):
        block = lax.rem(level + groups - d, groups) * plane + place
        return remote(
            packs.at[block, core], packs.at[block, core], z_send.at[d], z_recv.at[d],
            (block, core),
        )

    def p_copy(d, far):
        block = lax.rem(level + groups - d, groups) * plane + place
        return remote(
            packs.at[block, core], packs.at[block, core], p_send.at[d * plane + far],
            p_recv.at[d * plane + far],
            (level * plane + lax.rem(place + far, plane), core),
        )

    def p_arrival(d, far):
        origin = lax.rem(place + plane - far, plane)
        block = lax.rem(level + groups - d, groups) * plane + origin
        return remote(
            packs.at[block, core], packs.at[block, core], p_send.at[d * plane + far],
            p_recv.at[d * plane + far], (level * plane + origin, core),
        )

    def t_copy(d, far, part):
        origin = lax.rem(place + plane - far, plane)
        block = lax.rem(level + groups - d, groups) * plane + origin
        return remote(
            packs.at[block, part], packs.at[block, part], t_send.at[d * plane + far],
            t_recv.at[d * plane + far], (index, 1 - core),
        )

    def wanted(d, far, sender):
        ahead = lax.rem(place + far, plane) > place if sender else place >= far
        live = level >= d
        if d == 0:
            return live & ahead
        if d == reach:
            return live & jnp.logical_not(ahead)
        return live

    for d in range(1, reach + 1):
        pl.when(level + d < groups)(lambda d=d: z_copy(d).start())
    for far in range(1, plane):
        pl.when(wanted(0, far, True))(lambda far=far: p_copy(0, far).start())

    for copy in loads[2:5]:
        copy.wait()
    blank = jnp.zeros((HEAD_LANES - per_head, rows), jnp.bfloat16)
    for h in range(heads):
        own = query[h * per_head : (h + 1) * per_head, :]
        plain, moved = own[:UNROTATED_DIM], turn(own[UNROTATED_DIM:], cosine, sine)
        parts = [plain, moved, blank] if h % 2 == 0 else [moved, blank, plain]
        turned[h] = jnp.concatenate(parts, axis=0)
    wv_turned[...] = wv[...].astype(jnp.float32).T.astype(jnp.bfloat16)
    power = per_head ** (-0.5) * math.log2(math.e)

    def attend(block, first):
        source = jnp.concatenate([packs[block, part, :half, :] for part in range(2)], axis=0)
        tail = jnp.concatenate(
            [
                jnp.concatenate([packs[block, part, half:, :half] for part in range(2)], axis=1),
                jnp.concatenate(
                    [packs[block, part, half : half + 16, half : 2 * half] for part in range(2)], axis=1
                ),
            ],
            axis=0,
        )
        shape = (ROPE + 16, 3 * HEAD_LANES)
        line = lax.broadcasted_iota(jnp.int32, shape, 0)
        lane = lax.broadcasted_iota(jnp.int32, shape, 1)
        keyed = (line < ROPE) & ((lane == line + UNROTATED_DIM) | (lane == line + 2 * HEAD_LANES))
        named = (line == ROPE) & (lane >= HEAD_LANES) & (lane < 2 * HEAD_LANES)
        chooser = jnp.where(keyed | named, 1.0, 0.0).astype(jnp.bfloat16)
        extra = lax.dot_general(
            tail, chooser, (((0,), (0,)), ((), ())), preferred_element_type=jnp.float32
        )
        extras = [
            extra[:, :HEAD_LANES].astype(jnp.bfloat16), extra[:, 2 * HEAD_LANES :].astype(jnp.bfloat16)
        ]
        theirs = extra[:, HEAD_LANES : 2 * HEAD_LANES]
        theirs = jnp.concatenate([theirs] * (rows // HEAD_LANES), axis=1)
        live = theirs == docs
        if first:
            live = live & (
                lax.broadcasted_iota(jnp.int32, (rows, rows), 0)
                <= lax.broadcasted_iota(jnp.int32, (rows, rows), 1)
            )
        bias = jnp.where(live, 0.0, -1e30)
        keys = jnp.dot(source, wk[...], preferred_element_type=jnp.float32).astype(jnp.bfloat16)
        values = lax.dot_general(
            wv_turned[...], source, (((1,), (1,)), ((), ())), preferred_element_type=jnp.float32
        ).astype(jnp.bfloat16)
        side = lax.broadcasted_iota(jnp.int32, (rows, HEAD_LANES), 1) < UNROTATED_DIM
        for h in range(heads):
            low = h // 2 * HEAD_LANES
            pair = keys[:, low : low + HEAD_LANES]
            key = jnp.where(side, pair, extras[0]) if h % 2 == 0 else jnp.where(side, extras[1], pair)
            scores = jnp.dot(key, turned[h], preferred_element_type=jnp.float32) + bias
            top = jnp.max(scores, axis=0, keepdims=True)
            if not first:
                old = high[h : h + 1, :]
                top = jnp.maximum(old, top)
            weights = jnp.exp2((scores - top) * power)
            mass = jnp.sum(weights, axis=0, keepdims=True)
            mixed = jnp.dot(
                values[h * VALUE_ENTRIES : (h + 1) * VALUE_ENTRIES], weights.astype(jnp.bfloat16),
                preferred_element_type=jnp.float32,
            )
            high[h : h + 1, :] = top
            if first:
                total[h : h + 1, :] = mass
                acc[h] = mixed
            else:
                factor = jnp.exp2((old - top) * power)
                total[h : h + 1, :] = total[h : h + 1, :] * factor + mass
                acc[h] = acc[h] * factor + mixed

    attend(index, True)
    for d in range(1, reach + 1):

        def arrived(d=d):
            z_arrival(d).wait_recv()
            t_copy(d, 0, core).start()

        pl.when(level >= d)(arrived)
        for far in range(1, plane):
            pl.when(wanted(d, far, True))(lambda d=d, far=far: p_copy(d, far).start())

    def where_is(t):
        block = index - t
        d = level - block // plane
        far = lax.rem(place + plane - lax.rem(block, plane), plane)
        return block, d, far

    def pass_on(t):
        block, d, far = where_is(t)

        def passed():
            p_arrival(d, far).wait_recv()
            t_copy(d, far, core).start()

        pl.when(far > 0)(passed)

    last = jnp.minimum(index, reach * plane)
    pl.when(last > 0)(lambda: pass_on(1))

    def step(t, carry):
        pl.when(t < last)(lambda: pass_on(t + 1))
        block, d, far = where_is(t)
        t_copy(d, far, 1 - core).wait_recv()
        attend(block, False)
        return carry

    lax.fori_loop(1, last + 1, step, 0)

    for h in range(heads):
        done = (acc[h] / total[h : h + 1, :]).astype(jnp.bfloat16)
        for part in range(2):
            halves[part, h * VALUE_ENTRIES : (h + 1) * VALUE_ENTRIES, :] = done[:, part * half : (part + 1) * half]
    swap = remote(halves.at[1 - core], full.at[core], x_send, x_recv, (index, 1 - core))
    swap.start()
    full[core] = halves[core]
    loads[5].wait()
    loads[6].wait()
    remote(halves.at[core], full.at[1 - core], x_send, x_recv, (index, 1 - core)).wait_recv()
    width = proj.shape[1]
    tile = math.gcd(width, 512)
    attended = full[...].reshape(proj.shape[0], half).astype(jnp.float32).T.astype(jnp.bfloat16)

    def project(j, carry):
        columns = pl.ds(pl.multiple_of(j * tile, tile), tile)
        mix[:, columns] = jnp.dot(attended, proj[:, columns], preferred_element_type=jnp.float32)
        return carry

    lax.fori_loop(0, width // tile, project, 0)

    def settle(j, carry):
        some = pl.ds(pl.multiple_of(j * 16, 16), 16)
        branch = rms_scale(mix[some, :], mix_gain_ref[...])
        middle = (residual[some, :].astype(jnp.float32) + branch).astype(jnp.bfloat16)
        middle_ref[some, :] = middle
        normed[some, :] = rms_scale(middle.astype(jnp.float32), moe_gain_ref[...]).astype(jnp.bfloat16)
        return carry

    lax.fori_loop(0, half // 16, settle, 0)
    slots = grouped_ref.shape[0]
    chooser = jnp.where(
        lax.broadcasted_iota(jnp.int32, (slots, half), 0) == member_ref[...], 1.0, 0.0
    ).astype(jnp.bfloat16)

    def group(j, carry):
        columns = pl.ds(pl.multiple_of(j * tile, tile), tile)
        grouped_ref[:, columns] = jnp.dot(
            chooser, normed[:, columns], preferred_element_type=jnp.float32
        ).astype(jnp.bfloat16)
        return carry

    lax.fori_loop(0, width // tile, group, 0)

    swap.wait_send()
    for d in range(reach + 1):
        for far in range(0 if d else 1, plane):
            pl.when((level >= d) if far == 0 else wanted(d, far, False))(
                lambda d=d, far=far: t_copy(d, far, core).wait_send()
            )
            if far:
                pl.when(wanted(d, far, True))(lambda d=d, far=far: p_copy(d, far).wait_send())
    for d in range(1, reach + 1):
        pl.when(level + d < groups)(lambda d=d: z_copy(d).wait_send())


def attend(
    queries, latent, rope_key, wk, wv, proj, residual, cosine, sine, docs, member,
    mix_gain, moe_gain, count, slots,
):
    rows, rank = latent.shape
    half = rows // 2
    plane = count // GROUPS
    heads = wk.shape[1] // UNROTATED_DIM
    width = proj.shape[1]
    vmem = pl.BlockSpec(memory_space=pltpu.VMEM)
    hbm = pl.BlockSpec(memory_space=pl.ANY)
    dma = pltpu.SemaphoreType.DMA
    few, many = dma((GROUPS,)), dma((GROUPS * plane,))

    def held(*shape, dtype=jnp.bfloat16):
        return pltpu.VMEM(shape, dtype)

    loaded = (queries.T, latent, rope_key.T, wk, wv, proj, residual)
    return pl.pallas_call(
        functools.partial(attend_kernel, GROUPS, plane, heads),
        out_shape=(
            jax.ShapeDtypeStruct((half, width), jnp.bfloat16),
            jax.ShapeDtypeStruct((slots, width), jnp.bfloat16),
        ),
        in_specs=[hbm] * 7 + [vmem] * 6,
        out_specs=(vmem, vmem),
        scratch_shapes=[held(*array.shape) for array in loaded] + [
            held(count, 2, half + ROPE, rank),
            held(heads, HEAD_LANES, rows),
            held(heads * VALUE_ENTRIES, rank),
            held(heads, rows, dtype=jnp.float32),
            held(heads, rows, dtype=jnp.float32),
            held(heads, VALUE_ENTRIES, rows, dtype=jnp.float32),
            held(2, heads * VALUE_ENTRIES, half),
            held(2, heads * VALUE_ENTRIES, half),
            held(half, width, dtype=jnp.float32),
            held(half, width),
            dma((7,)), few, few, many, many, many, many, dma, dma,
        ],
        compiler_params=pltpu.CompilerParams(
            collective_id=3, has_side_effects=True, vmem_limit_bytes=40 * 1024 * 1024
        ),
        name="attend",
    )(
        *loaded, cosine, sine, docs, member, mix_gain[None, :], moe_gain[None, :],
    )


def local(
    residual,
    queries,
    latent,
    rope_key,
    doc_ids,
    latent_to_key,
    latent_to_value,
    out_proj,
    mix_gain,
    moe_gain,
    expert_ids,
    route_weight,
    gate_weight,
    up_weight,
    down_weight,
):
    local_rows = queries.shape[0]
    positions = lax.axis_index("sp") * local_rows + jnp.arange(local_rows, dtype=jnp.int32)
    cosine, sine = angles_of(positions)
    row_count, width = residual.shape
    top_count = expert_ids.shape[1]
    expert_count = lax.axis_size("sp")
    capacity = row_count // (expert_count // GROUPS)
    plane = expert_count // GROUPS
    group_rows = capacity * plane // top_count
    group_of = expert_ids[:, 0] // plane
    bins = jnp.arange(expert_count + GROUPS, dtype=jnp.int32)[None, :]
    group_bin = group_of[:, None] + expert_count
    named = jnp.any(expert_ids[:, :, None] == bins[None], axis=1) | (group_bin == bins)
    before = jnp.arange(row_count)[:, None] > jnp.arange(row_count)[None, :]
    earlier = jnp.dot(
        before.astype(jnp.bfloat16), named.astype(jnp.bfloat16), preferred_element_type=jnp.float32
    ).astype(jnp.int32)
    slot_rank = jnp.sum(jnp.where(expert_ids[:, :, None] == bins[None], earlier[:, None], 0), axis=2)
    group_rank = jnp.sum(jnp.where(group_bin == bins, earlier, 0), axis=1)
    slots = lax.rem(expert_ids, plane) * capacity + slot_rank
    member = (group_of * group_rows + group_rank)[:, None]
    chooser = (member == jnp.arange(GROUPS * group_rows, dtype=jnp.int32)[None, :]).astype(
        jnp.bfloat16
    )
    coarse = route_weight.astype(jnp.bfloat16)
    fine = (route_weight - coarse.astype(jnp.float32)).astype(jnp.bfloat16)
    fields = jnp.concatenate(
        [
            (slots + 1).astype(jnp.bfloat16),
            jnp.stack([coarse[:, 0], fine[:, 0], coarse[:, 1], fine[:, 1]], axis=1),
        ],
        axis=1,
    )
    fields = jnp.pad(fields, ((0, 0), (0, 16 - fields.shape[1])))
    meta = lax.dot_general(
        fields, chooser, (((0,), (0,)), ((), ())), preferred_element_type=jnp.float32
    )
    meta = meta - (jnp.arange(16) < top_count)[:, None].astype(jnp.float32)
    meta = meta.astype(jnp.bfloat16).reshape(16, GROUPS, group_rows).transpose(1, 0, 2)
    meta = jnp.pad(meta, ((0, 0), (0, 0), (0, -group_rows % 128)))
    middle, grouped = attend(
        queries, latent, rope_key, latent_to_key, latent_to_value, out_proj, residual,
        cosine, sine, doc_ids.astype(jnp.float32)[None, :], member[:, 0][None, :],
        mix_gain, moe_gain, expert_count, GROUPS * group_rows,
    )
    returned = run_experts(
        grouped.reshape(GROUPS, group_rows, width), meta, gate_weight[0], up_weight[0],
        down_weight[0], plane, capacity,
    )
    expert_mix = jnp.dot(
        chooser, returned.reshape(-1, width), preferred_element_type=jnp.float32
    )
    return (middle.astype(jnp.float32) + expert_mix).astype(jnp.bfloat16)


def solution(mesh):
    in_specs = (
        P(("sp", "tp"), None),
        P("sp", "tp"),
        P("sp", None),
        P("sp", None),
        P("sp"),
        P(None, "tp"),
        P(None, "tp"),
        P(),
        P(),
        P(),
        P(("sp", "tp"), None),
        P(("sp", "tp"), None),
        P("sp", None, "tp"),
        P("sp", None, "tp"),
        P("sp", "tp", None),
    )
    out_specs = P(("sp", "tp"), None)
    return jax.shard_map(local, mesh=mesh, in_specs=in_specs, out_specs=out_specs, check_vma=False)
```

```python
import functools
import math

import jax
import jax.numpy as jnp
from jax import lax
from jax.experimental import pallas as pl
from jax.experimental.pallas import tpu as pltpu
from jax.sharding import PartitionSpec as P

UNROTATED_DIM = 64
ROPE = 32
VALUE_ENTRIES = 64
GROUPS = 4
HEAD_LANES = 128
VMEM_GRANT = 56 * 1024 * 1024
PARTS = 2
OUTER = "out1 over0 ffn0 over1"
OUTER_MORE = ["back0 ffn1 out2 out3", "over2 ffn2 back2 over3", "ffn3 back3 back1 comb2", "comb3 comb1 comb0"]
INNER = "out1 out2 over0 ffn0"
INNER_MORE = ["over1 ffn1 back1 out3", "over2 ffn2 back2 comb1", "over3 ffn3 back3 back0", "comb2 comb3 comb0"]
MESH = pl.DeviceIdType.MESH

rope_base = 10000.0
epsilon = 1e-06


def angles_of(positions):
    half_width = ROPE // 2
    frequency = rope_base ** (-jnp.arange(half_width, dtype=jnp.float32) / half_width)
    angles = frequency[:, None] * positions.astype(jnp.float32)[None, :]
    return jnp.cos(angles), jnp.sin(angles)


def rms_scale(source, gain):
    return source * lax.rsqrt(jnp.mean(source * source, axis=-1, keepdims=True) + epsilon) * gain


def turn(pair, cosine, sine):
    half = ROPE // 2
    upper, lower = pair[:half].astype(jnp.float32), pair[half:].astype(jnp.float32)
    return jnp.concatenate(
        [upper * cosine - lower * sine, lower * cosine + upper * sine], axis=0
    ).astype(jnp.bfloat16)


def greet(groups, plane, meanwhile=None):
    index, core = lax.axis_index("sp"), lax.axis_index("tp")
    level, place = index // plane, lax.rem(index, plane)
    barrier = pltpu.get_barrier_semaphore()
    peers = [(lax.rem(level + d, groups) * plane + place, core) for d in range(1, groups)]
    peers += [(level * plane + lax.rem(place + d, plane), core) for d in range(1, plane)]
    peers += [(index, 1 - core)]
    for peer in peers:
        pl.semaphore_signal(barrier, inc=1, device_id=peer, device_id_type=MESH)
    if meanwhile is not None:
        meanwhile(index, core)
    pl.semaphore_wait(barrier, len(peers))
    return index, core, level, place


def remote(source, target, send_sem, recv_sem, peer):
    return pltpu.make_async_remote_copy(
        src_ref=source, dst_ref=target, send_sem=send_sem, recv_sem=recv_sem,
        device_id=peer, device_id_type=MESH,
    )


def level_order(groups):
    return sorted(range(groups), key=lambda d: min(d, groups - d))


def nearest(level, groups, at):
    picked = 0
    for l in range(groups):
        choice = sorted(range(groups), key=lambda s: (abs(s - l), s))[at]
        picked = picked + jnp.where(level == l, choice, 0)
    return picked


def expert_stage(
    groups, plane, where, ready, grouped, metas, out_ref,
    gate, up, down, landed, spread, arrived, hidden, partial, passed, mixed, back, merged,
    m_send, m_recv, z_send, z_recv, p_send, p_recv, own_sem, t_send, t_recv,
    x_send, x_recv, b_send, b_recv, keep_sem, r_send, r_recv,
):
    index, core, level, place = where
    started = []
    group_rows, width = grouped.shape[1:]
    capacity = spread.shape[2]
    slots = plane * capacity
    cut = width // PARTS
    source_of = [nearest(level, groups, k) for k in range(groups)]

    def begin(copy):
        copy.start()
        started.append(copy)

    def z_copy(k):
        other = source_of[k]
        return remote(
            grouped.at[other], landed.at[level], z_send.at[k], z_recv.at[level],
            (other * plane + place, core),
        )

    def out_copies(k):
        copies = []
        for far in range(plane - 1, 0, -1):
            to = lax.rem(place + far, plane)
            copies.append(remote(
                spread.at[k, to], arrived.at[k, core, place],
                p_send.at[k * plane + far], p_recv.at[k * plane + place],
                (level * plane + to, core),
            ))
        return copies

    def own_copy(k):
        return pltpu.make_async_copy(
            spread.at[k, place], arrived.at[k, core, place], own_sem.at[k]
        )

    def send_out(k):
        source = source_of[k]
        if k == 0:
            rows = grouped[level]
        else:
            peer = (source * plane + place, core)
            remote(metas.at[source], metas.at[source], m_send.at[k], m_recv.at[source], peer).wait_recv()
            remote(grouped.at[source], landed.at[source], z_send.at[k], z_recv.at[source], peer).wait_recv()
            rows = landed[source]
        info = metas[source][:, :group_rows].astype(jnp.float32)
        slot = lax.broadcasted_iota(jnp.int32, (slots, group_rows), 0).astype(jnp.float32)
        chooser = jnp.where((slot == info[0:1]) | (slot == info[1:2]), 1.0, 0.0)
        picked = jnp.dot(chooser.astype(jnp.bfloat16), rows, preferred_element_type=jnp.float32)
        for e in range(plane):
            spread[k, e] = picked[e * capacity : (e + 1) * capacity].astype(jnp.bfloat16)
        for copy in out_copies(k):
            copy.start()
        own_copy(k).start()

    def hand_over(k):
        for far in range(plane):
            origin = lax.rem(place + plane - far, plane)
            if far:
                remote(
                    spread.at[k, origin], arrived.at[k, core, origin],
                    p_send.at[k * plane + far], p_recv.at[k * plane + origin],
                    (level * plane + origin, core),
                ).wait_recv()
            else:
                own_copy(k).wait()
            begin(remote(
                arrived.at[k, core, origin], arrived.at[k, core, origin],
                t_send.at[k * plane + far], t_recv.at[k * plane + origin], (index, 1 - core),
            ))

    def experts(k):
        for origin in range(plane):
            remote(
                arrived.at[k, 1 - core, origin], arrived.at[k, 1 - core, origin],
                t_send.at[k * plane], t_recv.at[k * plane + origin], (index, 1 - core),
            ).wait_recv()
        units = gate.shape[1]
        unit_tile = math.gcd(units, 256)
        tile = math.gcd(cut, 256)

        def hide(j, carry):
            columns = pl.ds(pl.multiple_of(j * unit_tile, unit_tile), unit_tile)
            rows = arrived[k].reshape(2 * slots, width)
            gated = jnp.dot(rows, gate[:, columns], preferred_element_type=jnp.float32)
            raised = jnp.dot(rows, up[:, columns], preferred_element_type=jnp.float32)
            hidden[:, columns] = (gated / (1.0 + jnp.exp(-gated)) * raised).astype(jnp.bfloat16)
            return carry

        with jax.named_scope(f"E_hide{k}"):
            lax.fori_loop(0, units // unit_tile, hide, 0)
        for part in range(PARTS):

            def lower(j, carry, part=part):
                offset = pl.multiple_of(j * tile, tile)
                columns = pl.ds(pl.multiple_of(part * cut + offset, tile), tile)
                piece = jnp.dot(hidden[...], down[:, columns], preferred_element_type=jnp.float32)
                partial[k, part, :, :, :, pl.ds(offset, tile)] = piece.reshape(
                    2, plane, capacity, tile
                ).astype(jnp.bfloat16)
                return carry

            with jax.named_scope(f"E_lower{k}"):
                lax.fori_loop(0, cut // tile, lower, 0)
            at = k * PARTS + part
            begin(remote(
                partial.at[k, part, 1 - core], passed.at[k, part], x_send.at[at], x_recv.at[at],
                (index, 1 - core),
            ))

    def keep_copy(k, part):
        return pltpu.make_async_copy(
            mixed.at[k, part, place], back.at[k, part, place], keep_sem.at[k * PARTS + part]
        )

    def send_back(k):
        for part in range(PARTS):
            at = k * PARTS + part
            remote(
                partial.at[k, part, core], passed.at[k, part], x_send.at[at], x_recv.at[at],
                (index, 1 - core),
            ).wait_recv()
            for e in range(plane):
                mixed[k, part, e] = (
                    partial[k, part, core, e].astype(jnp.float32) + passed[k, part, e].astype(jnp.float32)
                ).astype(jnp.bfloat16)
            for far in range(plane - 1, 0, -1):
                to = lax.rem(place + far, plane)
                begin(remote(
                    mixed.at[k, part, to], back.at[k, part, place],
                    b_send.at[at * plane + far], b_recv.at[at * plane + place],
                    (level * plane + to, core),
                ))
            keep_copy(k, part).start()

    def combine(k):
        source = source_of[k]
        info = metas[source][:, :group_rows].astype(jnp.float32)
        slot = lax.broadcasted_iota(jnp.int32, (slots, group_rows), 0).astype(jnp.float32)
        hit_first, hit_second = slot == info[0:1], slot == info[1:2]
        for part in range(PARTS):
            at = k * PARTS + part
            for far in range(1, plane):
                origin = lax.rem(place + plane - far, plane)
                remote(
                    mixed.at[k, part, origin], back.at[k, part, origin],
                    b_send.at[at * plane + far], b_recv.at[at * plane + origin],
                    (level * plane + origin, core),
                ).wait_recv()
            keep_copy(k, part).wait()
            returned = back[k, part].reshape(slots, cut)
            result = 0.0
            for term in range(2):
                share = jnp.where(hit_first, info[2 + term : 3 + term], 0.0) + jnp.where(
                    hit_second, info[4 + term : 5 + term], 0.0
                )
                result = result + lax.dot_general(
                    share.astype(jnp.bfloat16), returned, (((0,), (0,)), ((), ())),
                    preferred_element_type=jnp.float32,
                )
            columns = slice(part * cut, (part + 1) * cut)
            if k == 0:
                out_ref[level, :, columns] = result.astype(jnp.bfloat16)
            else:
                merged[k, part] = result.astype(jnp.bfloat16)
                begin(remote(
                    merged.at[k, part], out_ref.at[level, :, columns],
                    r_send.at[at], r_recv.at[level * PARTS + part], (source * plane + place, core),
                ))

    steps = dict(out=send_out, over=hand_over, ffn=experts, back=send_back, comb=combine)

    def staged(name):
        with jax.named_scope("E_" + name):
            steps[name[:-1]](int(name[-1]))

    def finish(order):
        for name in " ".join(order).split():
            staged(name)
        with jax.named_scope("E_rest"):
            for k in range(1, groups):
                other = source_of[k]
                for part in range(PARTS):
                    at = k * PARTS + part
                    remote(
                        merged.at[k, part], out_ref.at[other, :, part * cut : (part + 1) * cut],
                        r_send.at[at], r_recv.at[other * PARTS + part], (other * plane + place, core),
                    ).wait_recv()
        for copy in started:
            copy.wait_send()
        started.clear()

    for k in (1, 0, 2, 3):
        ready(source_of[k])
        if k:
            z_copy(k).start()
        else:
            staged("out0")
    inner = (level > 0) & (level < groups - 1)
    pl.when(inner)(lambda: finish([INNER] + INNER_MORE))
    pl.when(jnp.logical_not(inner))(lambda: finish([OUTER] + OUTER_MORE))
    for k in range(groups):
        if k:
            z_copy(k).wait_send()
        for copy in out_copies(k):
            copy.wait_send()


def assign(groups, plane, expert_ids, route, meta_ref):
    row_count = expert_ids.shape[1]
    count = groups * plane
    capacity = row_count // plane
    group_rows = row_count // 2
    ids = expert_ids.astype(jnp.float32)
    first, second = ids[0:1], ids[1:2]
    bins = -(-(count + groups) // 16) * 16
    line = lax.broadcasted_iota(jnp.int32, (bins, row_count), 0).astype(jnp.float32)
    group = jnp.zeros_like(first)
    for g in range(1, groups):
        group = group + jnp.where(first >= g * plane, 1.0, 0.0)
    hit_first, hit_second = line == first, line == second
    hit_group = line == group + count
    named = jnp.where(hit_first | hit_second | hit_group, 1.0, 0.0).astype(jnp.bfloat16)
    square = (row_count, row_count)
    before = jnp.where(
        lax.broadcasted_iota(jnp.int32, square, 0) < lax.broadcasted_iota(jnp.int32, square, 1), 1.0, 0.0
    ).astype(jnp.bfloat16)
    earlier = jnp.dot(named, before, preferred_element_type=jnp.float32)

    def rank_of(hit):
        return jnp.sum(jnp.where(hit, earlier, 0.0), axis=0, keepdims=True)

    member = group * group_rows + rank_of(hit_group)
    base = group * plane
    fields = [
        (first - base) * capacity + rank_of(hit_first) + 1.0,
        (second - base) * capacity + rank_of(hit_second) + 1.0,
    ]
    for term in range(2):
        weight = route[term : term + 1]
        coarse = weight.astype(jnp.bfloat16).astype(jnp.float32)
        fields += [coarse, weight - coarse]
    line = lax.broadcasted_iota(jnp.int32, (16, row_count), 0)
    table = jnp.zeros((16, row_count), jnp.float32)
    for at, field in enumerate(fields):
        table = jnp.where(line == at, field, table)
    table = table.astype(jnp.bfloat16)
    lanes = meta_ref.shape[2]
    spot = lax.broadcasted_iota(jnp.int32, (lanes, row_count), 0).astype(jnp.float32)
    free = jnp.where(lax.broadcasted_iota(jnp.int32, (16, lanes), 0) < 2, 1.0, 0.0)
    for g in range(groups):
        taken = (spot + g * group_rows == member) & (spot < group_rows)
        info = lax.dot_general(
            table, jnp.where(taken, 1.0, 0.0).astype(jnp.bfloat16), (((1,), (1,)), ((), ())),
            preferred_element_type=jnp.float32,
        )
        meta_ref[g] = (info - free).astype(jnp.bfloat16)
    return member


def layer_kernel(
    groups, plane, heads,
    query_hbm, latent_hbm, rope_hbm, wk_hbm, wv_hbm, proj_hbm, residual_hbm,
    ids_hbm, docs_hbm, route_hbm, mix_gain_hbm, moe_gain_hbm, gate_hbm, up_hbm, down_hbm,
    cos_ref, sin_ref, middle_ref, chooser_ref, out_ref,
    query, latent, rope, wk, wv, proj, residual, expert_ids, doc_ids, route, mix_gain, moe_gain,
    gate, up, down,
    packs, turned, wv_turned, high, total, acc, halves, full, mix, normed, grouped, meta, metas,
    load_sem, z_send, z_recv, p_send, p_recv, t_send, t_recv, x_send, x_recv, m_send, m_recv, *rest,
):
    loads = [
        pltpu.make_async_copy(source, target, load_sem.at[i])
        for i, (source, target) in enumerate([
            (latent_hbm, latent), (rope_hbm, rope), (docs_hbm, doc_ids), (query_hbm, query),
            (wk_hbm, wk), (wv_hbm, wv), (ids_hbm, expert_ids), (route_hbm, route),
            (mix_gain_hbm, mix_gain), (moe_gain_hbm, moe_gain), (residual_hbm, residual),
            (proj_hbm, proj), (gate_hbm, gate), (up_hbm, up), (down_hbm, down),
        ])
    ]
    for copy in loads:
        copy.start()
    rows = latent.shape[0]
    half = rows // 2
    per_head = UNROTATED_DIM + ROPE
    cosine, sine = cos_ref[...], sin_ref[...]

    def pack(index, core):
        for copy in loads[:3]:
            copy.wait()
        docs = doc_ids[...].astype(jnp.float32)
        key = turn(rope[...], cosine, sine)
        for part in range(2):
            span = slice(part * half, (part + 1) * half)
            packs[index, part, :half, :] = latent[span, :]
            line = lax.broadcasted_iota(jnp.int32, (ROPE, half), 0)
            ids = jnp.where(line == 0, jnp.broadcast_to(docs[:, span], (ROPE, half)), 0.0)
            packs[index, part, half:, :half] = key[:, span]
            packs[index, part, half:, half : 2 * half] = ids.astype(jnp.bfloat16)

    with jax.named_scope("A_greet"):
        index, core, level, place = greet(groups, plane, pack)
    reach = groups // 2

    def z_copy(d):
        return remote(
            packs.at[index, core], packs.at[index, core], z_send.at[d], z_recv.at[d],
            (lax.rem(level + d, groups) * plane + place, core),
        )

    def z_arrival(d):
        block = lax.rem(level + groups - d, groups) * plane + place
        return remote(
            packs.at[block, core], packs.at[block, core], z_send.at[d], z_recv.at[d],
            (block, core),
        )

    def p_copy(d, far):
        block = lax.rem(level + groups - d, groups) * plane + place
        return remote(
            packs.at[block, core], packs.at[block, core], p_send.at[d * plane + far],
            p_recv.at[d * plane + far],
            (level * plane + lax.rem(place + far, plane), core),
        )

    def p_arrival(d, far):
        origin = lax.rem(place + plane - far, plane)
        block = lax.rem(level + groups - d, groups) * plane + origin
        return remote(
            packs.at[block, core], packs.at[block, core], p_send.at[d * plane + far],
            p_recv.at[d * plane + far], (level * plane + origin, core),
        )

    def t_copy(d, far, part):
        origin = lax.rem(place + plane - far, plane)
        block = lax.rem(level + groups - d, groups) * plane + origin
        return remote(
            packs.at[block, part], packs.at[block, part], t_send.at[d * plane + far],
            t_recv.at[d * plane + far], (index, 1 - core),
        )

    def wanted(d, far, sender):
        ahead = lax.rem(place + far, plane) > place if sender else place >= far
        live = level >= d
        if d == 0:
            return live & ahead
        if d == reach:
            return live & jnp.logical_not(ahead)
        return live

    for d in range(1, reach + 1):
        pl.when(level + d < groups)(lambda d=d: z_copy(d).start())
    for far in range(1, plane):
        pl.when(wanted(0, far, True))(lambda far=far: p_copy(0, far).start())

    for copy in loads[3:10]:
        copy.wait()
    docs = doc_ids[...].astype(jnp.float32)
    with jax.named_scope("A_assign"):
        member = assign(groups, plane, expert_ids[...], route[...], meta)
    metas[level] = meta[level]

    def m_copy(k):
        other = nearest(level, groups, k)
        return remote(
            meta.at[other], metas.at[level], m_send.at[k], m_recv.at[level],
            (other * plane + place, core),
        )

    for k in range(1, groups):
        m_copy(k).start()
    blank = jnp.zeros((HEAD_LANES - per_head, rows), jnp.bfloat16)
    for h in range(heads):
        own = query[h * per_head : (h + 1) * per_head, :]
        plain, moved = own[:UNROTATED_DIM], turn(own[UNROTATED_DIM:], cosine, sine)
        parts = [plain, moved, blank] if h % 2 == 0 else [moved, blank, plain]
        turned[h] = jnp.concatenate(parts, axis=0)
    wv_turned[...] = wv[...].astype(jnp.float32).T.astype(jnp.bfloat16)
    power = per_head ** (-0.5) * math.log2(math.e)

    def attend(block, first):
        source = jnp.concatenate([packs[block, part, :half, :] for part in range(2)], axis=0)
        tail = jnp.concatenate(
            [
                jnp.concatenate([packs[block, part, half:, :half] for part in range(2)], axis=1),
                jnp.concatenate(
                    [packs[block, part, half : half + 16, half : 2 * half] for part in range(2)], axis=1
                ),
            ],
            axis=0,
        )
        shape = (ROPE + 16, 3 * HEAD_LANES)
        line = lax.broadcasted_iota(jnp.int32, shape, 0)
        lane = lax.broadcasted_iota(jnp.int32, shape, 1)
        keyed = (line < ROPE) & ((lane == line + UNROTATED_DIM) | (lane == line + 2 * HEAD_LANES))
        named = (line == ROPE) & (lane >= HEAD_LANES) & (lane < 2 * HEAD_LANES)
        chooser = jnp.where(keyed | named, 1.0, 0.0).astype(jnp.bfloat16)
        extra = lax.dot_general(
            tail, chooser, (((0,), (0,)), ((), ())), preferred_element_type=jnp.float32
        )
        extras = [
            extra[:, :HEAD_LANES].astype(jnp.bfloat16), extra[:, 2 * HEAD_LANES :].astype(jnp.bfloat16)
        ]
        theirs = extra[:, HEAD_LANES : 2 * HEAD_LANES]
        theirs = jnp.concatenate([theirs] * (rows // HEAD_LANES), axis=1)
        live = theirs == docs
        if first:
            live = live & (
                lax.broadcasted_iota(jnp.int32, (rows, rows), 0)
                <= lax.broadcasted_iota(jnp.int32, (rows, rows), 1)
            )
        bias = jnp.where(live, 0.0, -1e30)
        keys = jnp.dot(source, wk[...], preferred_element_type=jnp.float32).astype(jnp.bfloat16)
        values = lax.dot_general(
            wv_turned[...], source, (((1,), (1,)), ((), ())), preferred_element_type=jnp.float32
        ).astype(jnp.bfloat16)
        side = lax.broadcasted_iota(jnp.int32, (rows, HEAD_LANES), 1) < UNROTATED_DIM
        for h in range(heads):
            low = h // 2 * HEAD_LANES
            pair = keys[:, low : low + HEAD_LANES]
            key = jnp.where(side, pair, extras[0]) if h % 2 == 0 else jnp.where(side, extras[1], pair)
            scores = jnp.dot(key, turned[h], preferred_element_type=jnp.float32) + bias
            top = jnp.max(scores, axis=0, keepdims=True)
            if not first:
                old = high[h : h + 1, :]
                top = jnp.maximum(old, top)
            weights = jnp.exp2((scores - top) * power)
            mass = jnp.sum(weights, axis=0, keepdims=True)
            mixed = jnp.dot(
                values[h * VALUE_ENTRIES : (h + 1) * VALUE_ENTRIES], weights.astype(jnp.bfloat16),
                preferred_element_type=jnp.float32,
            )
            high[h : h + 1, :] = top
            if first:
                total[h : h + 1, :] = mass
                acc[h] = mixed
            else:
                factor = jnp.exp2((old - top) * power)
                total[h : h + 1, :] = total[h : h + 1, :] * factor + mass
                acc[h] = acc[h] * factor + mixed

    with jax.named_scope("A_own"):
        attend(index, True)

    def relay(d):
        def arrived():
            with jax.named_scope(f"A_z{d}"):
                z_arrival(d).wait_recv()
            t_copy(d, 0, core).start()

        pl.when(level >= d)(arrived)
        for far in range(1, plane):
            pl.when(wanted(d, far, True))(lambda: p_copy(d, far).start())

    relay(1)

    def where_is(t):
        block = index - t
        d = level - block // plane
        far = lax.rem(place + plane - lax.rem(block, plane), plane)
        return block, d, far

    def pass_on(t):
        block, d, far = where_is(t)

        def passed():
            with jax.named_scope("A_pass"):
                p_arrival(d, far).wait_recv()
            t_copy(d, far, core).start()

        pl.when(far > 0)(passed)

    last = jnp.minimum(index, reach * plane)
    pl.when(last > 0)(lambda: pass_on(1))

    def step(t, carry):
        @pl.when(t == place + 1)
        def _():
            for d in range(2, reach + 1):
                relay(d)

        pl.when(t < last)(lambda: pass_on(t + 1))
        block, d, far = where_is(t)
        with jax.named_scope("A_wait"):
            t_copy(d, far, 1 - core).wait_recv()
        with jax.named_scope("A_block"):
            attend(block, False)
        return carry

    lax.fori_loop(1, last + 1, step, 0)

    for h in range(heads):
        done = (acc[h] / total[h : h + 1, :]).astype(jnp.bfloat16)
        for part in range(2):
            halves[part, h * VALUE_ENTRIES : (h + 1) * VALUE_ENTRIES, :] = done[:, part * half : (part + 1) * half]
    swap = remote(halves.at[1 - core], full.at[core], x_send, x_recv, (index, 1 - core))
    swap.start()
    full[core] = halves[core]
    loads[10].wait()
    loads[11].wait()
    with jax.named_scope("A_swap"):
        remote(halves.at[core], full.at[1 - core], x_send, x_recv, (index, 1 - core)).wait_recv()
    width = proj.shape[1]
    tile = math.gcd(width, 512)
    attended = full[...].reshape(proj.shape[0], half).astype(jnp.float32).T.astype(jnp.bfloat16)

    def project(j, carry):
        columns = pl.ds(pl.multiple_of(j * tile, tile), tile)
        mix[:, columns] = jnp.dot(attended, proj[:, columns], preferred_element_type=jnp.float32)
        return carry

    with jax.named_scope("A_project"):
        lax.fori_loop(0, width // tile, project, 0)

    def settle(j, carry):
        some = pl.ds(pl.multiple_of(j * 16, 16), 16)
        branch = rms_scale(mix[some, :], mix_gain[...])
        middle = (residual[some, :].astype(jnp.float32) + branch).astype(jnp.bfloat16)
        middle_ref[some, :] = middle
        normed[some, :] = rms_scale(middle.astype(jnp.float32), moe_gain[...]).astype(jnp.bfloat16)
        return carry

    with jax.named_scope("A_settle"):
        lax.fori_loop(0, half // 16, settle, 0, unroll=2)
    group_rows = grouped.shape[1]
    slots = groups * group_rows
    chooser_ref[...] = jnp.where(
        lax.broadcasted_iota(jnp.int32, (slots, half), 0).astype(jnp.float32) == member, 1.0, 0.0
    ).astype(jnp.bfloat16)

    def ready(group):
        picks = chooser_ref[pl.ds(pl.multiple_of(group * group_rows, group_rows), group_rows), :]
        for j in range(width // tile):
            columns = slice(j * tile, (j + 1) * tile)
            grouped[group, :, columns] = jnp.dot(
                picks, normed[:, columns], preferred_element_type=jnp.float32
            ).astype(jnp.bfloat16)

    for copy in loads[12:]:
        copy.wait()
    expert_stage(
        groups, plane, (index, core, level, place), ready, grouped, metas, out_ref,
        gate, up, down, *rest[:9], m_send, m_recv, *rest[9:],
    )

    swap.wait_send()
    for d in range(reach + 1):
        for far in range(0 if d else 1, plane):
            pl.when((level >= d) if far == 0 else wanted(d, far, False))(
                lambda d=d, far=far: t_copy(d, far, core).wait_send()
            )
            if far:
                pl.when(wanted(d, far, True))(lambda d=d, far=far: p_copy(d, far).wait_send())
    for d in range(1, reach + 1):
        pl.when(level + d < groups)(lambda d=d: z_copy(d).wait_send())
    for k in range(1, groups):
        m_copy(k).wait_send()


def layer(
    queries, latent, rope_key, wk, wv, proj, residual, expert_ids, doc_ids, route,
    mix_gain, moe_gain, gate, up, down, cosine, sine, count,
):
    rows, rank = latent.shape
    half = rows // 2
    plane = count // GROUPS
    capacity = half // plane
    heads = wk.shape[1] // UNROTATED_DIM
    width = proj.shape[1]
    units = gate.shape[1]
    group_rows = half // 2
    cut = width // PARTS
    vmem = pl.BlockSpec(memory_space=pltpu.VMEM)
    hbm = pl.BlockSpec(memory_space=pltpu.HBM)
    dma = pltpu.SemaphoreType.DMA
    few, many = dma((GROUPS,)), dma((GROUPS * plane,))
    few_parts, many_parts = dma((GROUPS * PARTS,)), dma((GROUPS * PARTS * plane,))

    def held(*shape, dtype=jnp.bfloat16):
        return pltpu.VMEM(shape, dtype)

    loaded = (
        queries.T, latent, rope_key.T, wk, wv, proj, residual, expert_ids.T, doc_ids[None, :],
        route.T, mix_gain[None, :], moe_gain[None, :], gate, up, down,
    )
    table = held(GROUPS, 16, -(-group_rows // 128) * 128)
    block = held(GROUPS, PARTS, plane, capacity, cut)
    return pl.pallas_call(
        functools.partial(layer_kernel, GROUPS, plane, heads),
        out_shape=(
            jax.ShapeDtypeStruct((half, width), jnp.bfloat16),
            jax.ShapeDtypeStruct((GROUPS * group_rows, half), jnp.bfloat16),
            jax.ShapeDtypeStruct((GROUPS, group_rows, width), jnp.bfloat16),
        ),
        in_specs=[hbm] * len(loaded) + [vmem] * 2,
        out_specs=(vmem,) * 3,
        scratch_shapes=[held(*array.shape, dtype=array.dtype) for array in loaded] + [
            held(count, 2, half + ROPE, rank),
            held(heads, HEAD_LANES, rows),
            held(heads * VALUE_ENTRIES, rank),
            held(heads, rows, dtype=jnp.float32),
            held(heads, rows, dtype=jnp.float32),
            held(heads, VALUE_ENTRIES, rows, dtype=jnp.float32),
            held(2, heads * VALUE_ENTRIES, half),
            held(2, heads * VALUE_ENTRIES, half),
            held(half, width, dtype=jnp.float32),
            held(half, width),
            held(GROUPS, group_rows, width), table, table,
            dma((len(loaded),)), few, few, many, many, many, many, dma, dma, few, few,
            held(GROUPS, group_rows, width),
            held(GROUPS, plane, capacity, width),
            held(GROUPS, 2, plane, capacity, width),
            held(2 * plane * capacity, units),
            held(GROUPS, PARTS, 2, plane, capacity, cut),
            block, block, block,
            held(GROUPS, PARTS, group_rows, cut),
            few, few, many, many, few, many, many,
            few_parts, few_parts, many_parts, many_parts, few_parts, few_parts, few_parts,
        ],
        compiler_params=pltpu.CompilerParams(
            collective_id=3, has_side_effects=True, vmem_limit_bytes=VMEM_GRANT
        ),
        name="layer",
    )(*loaded, cosine, sine)


def local(
    residual,
    queries,
    latent,
    rope_key,
    doc_ids,
    latent_to_key,
    latent_to_value,
    out_proj,
    mix_gain,
    moe_gain,
    expert_ids,
    route_weight,
    gate_weight,
    up_weight,
    down_weight,
):
    local_rows = queries.shape[0]
    positions = lax.axis_index("sp") * local_rows + jnp.arange(local_rows, dtype=jnp.int32)
    cosine, sine = angles_of(positions)
    middle, chooser, returned = layer(
        queries, latent, rope_key, latent_to_key, latent_to_value, out_proj, residual,
        expert_ids, doc_ids, route_weight, mix_gain, moe_gain, gate_weight[0], up_weight[0],
        down_weight[0], cosine, sine, lax.axis_size("sp"),
    )
    expert_mix = lax.dot_general(
        chooser, returned.reshape(chooser.shape[0], -1), (((0,), (0,)), ((), ())),
        preferred_element_type=jnp.float32,
    )
    return (middle.astype(jnp.float32) + expert_mix).astype(jnp.bfloat16)


def solution(mesh):
    in_specs = (
        P(("sp", "tp"), None),
        P("sp", "tp"),
        P("sp", None),
        P("sp", None),
        P("sp"),
        P(None, "tp"),
        P(None, "tp"),
        P(),
        P(),
        P(),
        P(("sp", "tp"), None),
        P(("sp", "tp"), None),
        P("sp", None, "tp"),
        P("sp", None, "tp"),
        P("sp", "tp", None),
    )
    out_specs = P(("sp", "tp"), None)
    return jax.shard_map(local, mesh=mesh, in_specs=in_specs, out_specs=out_specs, check_vma=False)
```

```python
import functools
import math

import jax
import jax.numpy as jnp
from jax import lax
from jax.experimental import pallas as pl
from jax.experimental.pallas import tpu as pltpu
from jax.sharding import PartitionSpec as P

UNROTATED_DIM = 64
ROPE = 32
VALUE_ENTRIES = 64
GROUPS = 4
HEAD_LANES = 128
VMEM_GRANT = 56 * 1024 * 1024
PARTS = 2
OUTER = "out1 over0 ffn0 over1"
OUTER_MORE = ["back0 ffn1 out2 out3", "over2 ffn2 back2 over3", "ffn3 back3 back1 comb2", "comb3 comb1 comb0"]
INNER = "out1 out2 over0 ffn0"
INNER_MORE = ["over1 ffn1 back1 out3", "over2 ffn2 back2 comb1", "over3 ffn3 back3 back0", "comb2 comb3 comb0"]
MESH = pl.DeviceIdType.MESH

rope_base = 10000.0
epsilon = 1e-06


def angles_of(first, count):
    half_width = ROPE // 2
    line = lax.broadcasted_iota(jnp.int32, (half_width, count), 0)
    frequency = jnp.zeros((half_width, count), jnp.float32)
    for i in range(half_width):
        frequency = jnp.where(line == i, rope_base ** (-i / half_width), frequency)
    positions = first + lax.broadcasted_iota(jnp.int32, (half_width, count), 1)
    angles = positions.astype(jnp.float32) * frequency
    return jnp.cos(angles), jnp.sin(angles)


def rms_scale(source, gain):
    return source * lax.rsqrt(jnp.mean(source * source, axis=-1, keepdims=True) + epsilon) * gain


def turn(pair, cosine, sine):
    half = ROPE // 2
    upper, lower = pair[:half].astype(jnp.float32), pair[half:].astype(jnp.float32)
    return jnp.concatenate(
        [upper * cosine - lower * sine, lower * cosine + upper * sine], axis=0
    ).astype(jnp.bfloat16)


def greet(groups, plane, meanwhile=None):
    index, core = lax.axis_index("sp"), lax.axis_index("tp")
    level, place = index // plane, lax.rem(index, plane)
    barrier = pltpu.get_barrier_semaphore()
    peers = [(lax.rem(level + d, groups) * plane + place, core) for d in range(1, groups)]
    peers += [(level * plane + lax.rem(place + d, plane), core) for d in range(1, plane)]
    peers += [(index, 1 - core)]
    for peer in peers:
        pl.semaphore_signal(barrier, inc=1, device_id=peer, device_id_type=MESH)
    if meanwhile is not None:
        meanwhile(index, core)
    pl.semaphore_wait(barrier, len(peers))
    return index, core, level, place


def remote(source, target, send_sem, recv_sem, peer):
    return pltpu.make_async_remote_copy(
        src_ref=source, dst_ref=target, send_sem=send_sem, recv_sem=recv_sem,
        device_id=peer, device_id_type=MESH,
    )


def level_order(groups):
    return sorted(range(groups), key=lambda d: min(d, groups - d))


def nearest(level, groups, at):
    picked = 0
    for l in range(groups):
        order = sorted(range(groups), key=lambda s: (abs(s - l), s))
        if l in (0, groups - 1):
            order[2:] = order[:1:-1]
        picked = picked + jnp.where(level == l, order[at], 0)
    return picked


def expert_stage(
    groups, plane, where, ready, grouped, metas, out_ref,
    gate, up, down, landed, spread, arrived, hidden, partial, passed, mixed, back, merged,
    m_send, m_recv, z_send, z_recv, p_send, p_recv, own_sem, t_send, t_recv,
    x_send, x_recv, b_send, b_recv, keep_sem, r_send, r_recv,
):
    index, core, level, place = where
    started = []
    group_rows, width = grouped.shape[1:]
    capacity = spread.shape[2]
    slots = plane * capacity
    cut = width // PARTS
    source_of = [nearest(level, groups, k) for k in range(groups)]

    def begin(copy):
        copy.start()
        started.append(copy)

    def z_copy(k):
        other = source_of[k]
        return remote(
            grouped.at[other], landed.at[level], z_send.at[k], z_recv.at[level],
            (other * plane + place, core),
        )

    def out_copies(k):
        copies = []
        for far in range(plane - 1, 0, -1):
            to = lax.rem(place + far, plane)
            copies.append(remote(
                spread.at[k, to], arrived.at[k, core, place],
                p_send.at[k * plane + far], p_recv.at[k * plane + place],
                (level * plane + to, core),
            ))
        return copies

    def own_copy(k):
        return pltpu.make_async_copy(
            spread.at[k, place], arrived.at[k, core, place], own_sem.at[k]
        )

    def send_out(k):
        source = source_of[k]
        if k == 0:
            rows = grouped[level]
        else:
            peer = (source * plane + place, core)
            remote(metas.at[source], metas.at[source], m_send.at[k], m_recv.at[source], peer).wait_recv()
            remote(grouped.at[source], landed.at[source], z_send.at[k], z_recv.at[source], peer).wait_recv()
            rows = landed[source]
        info = metas[source][:, :group_rows].astype(jnp.float32)
        slot = lax.broadcasted_iota(jnp.int32, (slots, group_rows), 0).astype(jnp.float32)
        chooser = jnp.where((slot == info[0:1]) | (slot == info[1:2]), 1.0, 0.0)
        picked = jnp.dot(chooser.astype(jnp.bfloat16), rows, preferred_element_type=jnp.float32)
        for e in range(plane):
            spread[k, e] = picked[e * capacity : (e + 1) * capacity].astype(jnp.bfloat16)
        for copy in out_copies(k):
            copy.start()
        own_copy(k).start()

    def hand_over(k):
        for far in range(plane):
            origin = lax.rem(place + plane - far, plane)
            if far:
                remote(
                    spread.at[k, origin], arrived.at[k, core, origin],
                    p_send.at[k * plane + far], p_recv.at[k * plane + origin],
                    (level * plane + origin, core),
                ).wait_recv()
            else:
                own_copy(k).wait()
            begin(remote(
                arrived.at[k, core, origin], arrived.at[k, core, origin],
                t_send.at[k * plane + far], t_recv.at[k * plane + origin], (index, 1 - core),
            ))

    def experts(k):
        for origin in range(plane):
            remote(
                arrived.at[k, 1 - core, origin], arrived.at[k, 1 - core, origin],
                t_send.at[k * plane], t_recv.at[k * plane + origin], (index, 1 - core),
            ).wait_recv()
        units = gate.shape[1]
        unit_tile = math.gcd(units, 256)
        tile = math.gcd(cut, 256)

        def hide(j, carry):
            columns = pl.ds(pl.multiple_of(j * unit_tile, unit_tile), unit_tile)
            rows = arrived[k].reshape(2 * slots, width)
            gated = jnp.dot(rows, gate[:, columns], preferred_element_type=jnp.float32)
            raised = jnp.dot(rows, up[:, columns], preferred_element_type=jnp.float32)
            hidden[:, columns] = (gated / (1.0 + jnp.exp(-gated)) * raised).astype(jnp.bfloat16)
            return carry

        with jax.named_scope(f"E_hide{k}"):
            lax.fori_loop(0, units // unit_tile, hide, 0)
        for part in range(PARTS):

            def lower(j, carry, part=part):
                offset = pl.multiple_of(j * tile, tile)
                columns = pl.ds(pl.multiple_of(part * cut + offset, tile), tile)
                piece = jnp.dot(hidden[...], down[:, columns], preferred_element_type=jnp.float32)
                partial[k, part, :, :, :, pl.ds(offset, tile)] = piece.reshape(
                    2, plane, capacity, tile
                ).astype(jnp.bfloat16)
                return carry

            with jax.named_scope(f"E_lower{k}"):
                lax.fori_loop(0, cut // tile, lower, 0)
            at = k * PARTS + part
            begin(remote(
                partial.at[k, part, 1 - core], passed.at[k, part], x_send.at[at], x_recv.at[at],
                (index, 1 - core),
            ))

    def keep_copy(k, part):
        return pltpu.make_async_copy(
            mixed.at[k, part, place], back.at[k, part, place], keep_sem.at[k * PARTS + part]
        )

    def send_back(k):
        for part in range(PARTS):
            at = k * PARTS + part
            remote(
                partial.at[k, part, core], passed.at[k, part], x_send.at[at], x_recv.at[at],
                (index, 1 - core),
            ).wait_recv()
            for e in range(plane):
                mixed[k, part, e] = (
                    partial[k, part, core, e].astype(jnp.float32) + passed[k, part, e].astype(jnp.float32)
                ).astype(jnp.bfloat16)
            for far in range(plane - 1, 0, -1):
                to = lax.rem(place + far, plane)
                begin(remote(
                    mixed.at[k, part, to], back.at[k, part, place],
                    b_send.at[at * plane + far], b_recv.at[at * plane + place],
                    (level * plane + to, core),
                ))
            keep_copy(k, part).start()

    def combine(k):
        source = source_of[k]
        info = metas[source][:, :group_rows].astype(jnp.float32)
        slot = lax.broadcasted_iota(jnp.int32, (slots, group_rows), 0).astype(jnp.float32)
        hit_first, hit_second = slot == info[0:1], slot == info[1:2]
        for part in range(PARTS):
            at = k * PARTS + part
            for far in range(1, plane):
                origin = lax.rem(place + plane - far, plane)
                remote(
                    mixed.at[k, part, origin], back.at[k, part, origin],
                    b_send.at[at * plane + far], b_recv.at[at * plane + origin],
                    (level * plane + origin, core),
                ).wait_recv()
            keep_copy(k, part).wait()
            returned = back[k, part].reshape(slots, cut)
            result = 0.0
            for term in range(2):
                share = jnp.where(hit_first, info[2 + term : 3 + term], 0.0) + jnp.where(
                    hit_second, info[4 + term : 5 + term], 0.0
                )
                result = result + lax.dot_general(
                    share.astype(jnp.bfloat16), returned, (((0,), (0,)), ((), ())),
                    preferred_element_type=jnp.float32,
                )
            columns = slice(part * cut, (part + 1) * cut)
            if k == 0:
                out_ref[level, :, columns] = result.astype(jnp.bfloat16)
            else:
                merged[k, part] = result.astype(jnp.bfloat16)
                begin(remote(
                    merged.at[k, part], out_ref.at[level, :, columns],
                    r_send.at[at], r_recv.at[level * PARTS + part], (source * plane + place, core),
                ))

    steps = dict(out=send_out, over=hand_over, ffn=experts, back=send_back, comb=combine)

    def staged(name):
        with jax.named_scope("E_" + name):
            steps[name[:-1]](int(name[-1]))

    def finish(order):
        for name in " ".join(order).split():
            staged(name)
        with jax.named_scope("E_rest"):
            for k in range(1, groups):
                other = source_of[k]
                for part in range(PARTS):
                    at = k * PARTS + part
                    remote(
                        merged.at[k, part], out_ref.at[other, :, part * cut : (part + 1) * cut],
                        r_send.at[at], r_recv.at[other * PARTS + part], (other * plane + place, core),
                    ).wait_recv()
        for copy in started:
            copy.wait_send()
        started.clear()

    for k in (1, 0, 2, 3):
        ready(source_of[k])
        if k:
            z_copy(k).start()
        else:
            staged("out0")
    inner = (level > 0) & (level < groups - 1)
    pl.when(inner)(lambda: finish([INNER] + INNER_MORE))
    pl.when(jnp.logical_not(inner))(lambda: finish([OUTER] + OUTER_MORE))
    for k in range(groups):
        if k:
            z_copy(k).wait_send()
        for copy in out_copies(k):
            copy.wait_send()


def assign(groups, plane, expert_ids, route, meta_ref):
    row_count = expert_ids.shape[1]
    count = groups * plane
    capacity = row_count // plane
    group_rows = row_count // 2
    ids = expert_ids.astype(jnp.float32)
    first, second = ids[0:1], ids[1:2]
    bins = -(-(count + groups) // 16) * 16
    line = lax.broadcasted_iota(jnp.int32, (bins, row_count), 0).astype(jnp.float32)
    group = jnp.zeros_like(first)
    for g in range(1, groups):
        group = group + jnp.where(first >= g * plane, 1.0, 0.0)
    hit_first, hit_second = line == first, line == second
    hit_group = line == group + count
    named = jnp.where(hit_first | hit_second | hit_group, 1.0, 0.0).astype(jnp.bfloat16)
    square = (row_count, row_count)
    before = jnp.where(
        lax.broadcasted_iota(jnp.int32, square, 0) < lax.broadcasted_iota(jnp.int32, square, 1), 1.0, 0.0
    ).astype(jnp.bfloat16)
    earlier = jnp.dot(named, before, preferred_element_type=jnp.float32)

    def rank_of(hit):
        return jnp.sum(jnp.where(hit, earlier, 0.0), axis=0, keepdims=True)

    member = group * group_rows + rank_of(hit_group)
    base = group * plane
    fields = [
        (first - base) * capacity + rank_of(hit_first) + 1.0,
        (second - base) * capacity + rank_of(hit_second) + 1.0,
    ]
    for term in range(2):
        weight = route[term : term + 1]
        coarse = weight.astype(jnp.bfloat16).astype(jnp.float32)
        fields += [coarse, weight - coarse]
    line = lax.broadcasted_iota(jnp.int32, (16, row_count), 0)
    table = jnp.zeros((16, row_count), jnp.float32)
    for at, field in enumerate(fields):
        table = jnp.where(line == at, field, table)
    table = table.astype(jnp.bfloat16)
    lanes = meta_ref.shape[2]
    spot = lax.broadcasted_iota(jnp.int32, (lanes, row_count), 0).astype(jnp.float32)
    free = jnp.where(lax.broadcasted_iota(jnp.int32, (16, lanes), 0) < 2, 1.0, 0.0)
    for g in range(groups):
        taken = (spot + g * group_rows == member) & (spot < group_rows)
        info = lax.dot_general(
            table, jnp.where(taken, 1.0, 0.0).astype(jnp.bfloat16), (((1,), (1,)), ((), ())),
            preferred_element_type=jnp.float32,
        )
        meta_ref[g] = (info - free).astype(jnp.bfloat16)
    return member


def layer_kernel(
    groups, plane, heads,
    query_hbm, latent_hbm, rope_hbm, wk_hbm, wv_hbm, proj_hbm, residual_hbm,
    ids_hbm, docs_hbm, route_hbm, mix_gain_hbm, moe_gain_hbm, gate_hbm, up_hbm, down_hbm,
    out_ref,
    query, latent, rope, wk, wv, proj, residual, expert_ids, doc_ids, route, mix_gain, moe_gain,
    gate, up, down, middle, chooser, returned,
    packs, turned, wv_turned, high, total, acc, halves, full, mix, normed, grouped, meta, metas,
    load_sem, z_send, z_recv, p_send, p_recv, t_send, t_recv, x_send, x_recv, m_send, m_recv, *rest,
):
    loads = [
        pltpu.make_async_copy(source, target, load_sem.at[i])
        for i, (source, target) in enumerate([
            (latent_hbm, latent), (rope_hbm, rope), (docs_hbm, doc_ids), (query_hbm, query),
            (wk_hbm, wk), (wv_hbm, wv), (ids_hbm, expert_ids), (route_hbm, route),
            (mix_gain_hbm, mix_gain), (moe_gain_hbm, moe_gain), (residual_hbm, residual),
            (proj_hbm, proj), (gate_hbm, gate), (up_hbm, up), (down_hbm, down),
        ])
    ]
    for copy in loads:
        copy.start()
    rows = latent.shape[0]
    half = rows // 2
    per_head = UNROTATED_DIM + ROPE
    cosine, sine = angles_of(lax.axis_index("sp") * rows, rows)

    def pack(index, core):
        for copy in loads[:3]:
            copy.wait()
        docs = doc_ids[...].astype(jnp.float32)
        key = turn(rope[...], cosine, sine)
        for part in range(2):
            span = slice(part * half, (part + 1) * half)
            packs[index, part, :half, :] = latent[span, :]
            line = lax.broadcasted_iota(jnp.int32, (ROPE, half), 0)
            ids = jnp.where(line == 0, jnp.broadcast_to(docs[:, span], (ROPE, half)), 0.0)
            packs[index, part, half:, :half] = key[:, span]
            packs[index, part, half:, half : 2 * half] = ids.astype(jnp.bfloat16)

    with jax.named_scope("A_greet"):
        index, core, level, place = greet(groups, plane, pack)
    reach = groups // 2

    def z_copy(d):
        return remote(
            packs.at[index, core], packs.at[index, core], z_send.at[d], z_recv.at[d],
            (lax.rem(level + d, groups) * plane + place, core),
        )

    def z_arrival(d):
        block = lax.rem(level + groups - d, groups) * plane + place
        return remote(
            packs.at[block, core], packs.at[block, core], z_send.at[d], z_recv.at[d],
            (block, core),
        )

    def p_copy(d, far):
        block = lax.rem(level + groups - d, groups) * plane + place
        return remote(
            packs.at[block, core], packs.at[block, core], p_send.at[d * plane + far],
            p_recv.at[d * plane + far],
            (level * plane + lax.rem(place + far, plane), core),
        )

    def p_arrival(d, far):
        origin = lax.rem(place + plane - far, plane)
        block = lax.rem(level + groups - d, groups) * plane + origin
        return remote(
            packs.at[block, core], packs.at[block, core], p_send.at[d * plane + far],
            p_recv.at[d * plane + far], (level * plane + origin, core),
        )

    def t_copy(d, far, part):
        origin = lax.rem(place + plane - far, plane)
        block = lax.rem(level + groups - d, groups) * plane + origin
        return remote(
            packs.at[block, part], packs.at[block, part], t_send.at[d * plane + far],
            t_recv.at[d * plane + far], (index, 1 - core),
        )

    def wanted(d, far, sender):
        ahead = lax.rem(place + far, plane) > place if sender else place >= far
        live = level >= d
        if d == 0:
            return live & ahead
        if d == reach:
            return live & jnp.logical_not(ahead)
        return live

    for d in range(1, reach + 1):
        pl.when(level + d < groups)(lambda d=d: z_copy(d).start())
    for far in range(1, plane):
        pl.when(wanted(0, far, True))(lambda far=far: p_copy(0, far).start())

    for copy in loads[3:10]:
        copy.wait()
    docs = doc_ids[...].astype(jnp.float32)
    with jax.named_scope("A_assign"):
        member = assign(groups, plane, expert_ids[...], route[...], meta)
    metas[level] = meta[level]

    def m_copy(k):
        other = nearest(level, groups, k)
        return remote(
            meta.at[other], metas.at[level], m_send.at[k], m_recv.at[level],
            (other * plane + place, core),
        )

    for k in range(1, groups):
        m_copy(k).start()
    blank = jnp.zeros((HEAD_LANES - per_head, rows), jnp.bfloat16)
    for h in range(heads):
        own = query[h * per_head : (h + 1) * per_head, :]
        plain, moved = own[:UNROTATED_DIM], turn(own[UNROTATED_DIM:], cosine, sine)
        parts = [plain, moved, blank] if h % 2 == 0 else [moved, blank, plain]
        turned[h] = jnp.concatenate(parts, axis=0)
    wv_turned[...] = wv[...].astype(jnp.float32).T.astype(jnp.bfloat16)
    power = per_head ** (-0.5) * math.log2(math.e)

    def attend(block, first):
        source = jnp.concatenate([packs[block, part, :half, :] for part in range(2)], axis=0)
        tail = jnp.concatenate(
            [
                jnp.concatenate([packs[block, part, half:, :half] for part in range(2)], axis=1),
                jnp.concatenate(
                    [packs[block, part, half : half + 16, half : 2 * half] for part in range(2)], axis=1
                ),
            ],
            axis=0,
        )
        shape = (ROPE + 16, 3 * HEAD_LANES)
        line = lax.broadcasted_iota(jnp.int32, shape, 0)
        lane = lax.broadcasted_iota(jnp.int32, shape, 1)
        keyed = (line < ROPE) & ((lane == line + UNROTATED_DIM) | (lane == line + 2 * HEAD_LANES))
        named = (line == ROPE) & (lane >= HEAD_LANES) & (lane < 2 * HEAD_LANES)
        chooser = jnp.where(keyed | named, 1.0, 0.0).astype(jnp.bfloat16)
        extra = lax.dot_general(
            tail, chooser, (((0,), (0,)), ((), ())), preferred_element_type=jnp.float32
        )
        extras = [
            extra[:, :HEAD_LANES].astype(jnp.bfloat16), extra[:, 2 * HEAD_LANES :].astype(jnp.bfloat16)
        ]
        theirs = extra[:, HEAD_LANES : 2 * HEAD_LANES]
        theirs = jnp.concatenate([theirs] * (rows // HEAD_LANES), axis=1)
        live = theirs == docs
        if first:
            live = live & (
                lax.broadcasted_iota(jnp.int32, (rows, rows), 0)
                <= lax.broadcasted_iota(jnp.int32, (rows, rows), 1)
            )
        bias = jnp.where(live, 0.0, -1e30)
        keys = jnp.dot(source, wk[...], preferred_element_type=jnp.float32).astype(jnp.bfloat16)
        values = lax.dot_general(
            wv_turned[...], source, (((1,), (1,)), ((), ())), preferred_element_type=jnp.float32
        ).astype(jnp.bfloat16)
        side = lax.broadcasted_iota(jnp.int32, (rows, HEAD_LANES), 1) < UNROTATED_DIM
        for h in range(heads):
            low = h // 2 * HEAD_LANES
            pair = keys[:, low : low + HEAD_LANES]
            key = jnp.where(side, pair, extras[0]) if h % 2 == 0 else jnp.where(side, extras[1], pair)
            scores = jnp.dot(key, turned[h], preferred_element_type=jnp.float32) + bias
            top = jnp.max(scores, axis=0, keepdims=True)
            if not first:
                old = high[h : h + 1, :]
                top = jnp.maximum(old, top)
            weights = jnp.exp2((scores - top) * power)
            mass = jnp.sum(weights, axis=0, keepdims=True)
            mixed = jnp.dot(
                values[h * VALUE_ENTRIES : (h + 1) * VALUE_ENTRIES], weights.astype(jnp.bfloat16),
                preferred_element_type=jnp.float32,
            )
            high[h : h + 1, :] = top
            if first:
                total[h : h + 1, :] = mass
                acc[h] = mixed
            else:
                factor = jnp.exp2((old - top) * power)
                total[h : h + 1, :] = total[h : h + 1, :] * factor + mass
                acc[h] = acc[h] * factor + mixed

    with jax.named_scope("A_own"):
        attend(index, True)

    def relay(d):
        def arrived():
            with jax.named_scope(f"A_z{d}"):
                z_arrival(d).wait_recv()
            t_copy(d, 0, core).start()

        pl.when(level >= d)(arrived)
        for far in range(1, plane):
            pl.when(wanted(d, far, True))(lambda: p_copy(d, far).start())

    relay(1)

    def where_is(t):
        below = t > place
        turn_at = jnp.where(below, t - place - 1, 0)
        d = jnp.where(below, 1 + turn_at // plane, 0)
        far = lax.rem(turn_at, plane)
        far = jnp.where((d == reach) & (far > 0), place + far, far)
        far = jnp.where(below, far, t)
        block = (level - d) * plane + lax.rem(place + plane - far, plane)
        return block, d, far

    def pass_on(t):
        block, d, far = where_is(t)

        def passed():
            with jax.named_scope("A_pass"):
                p_arrival(d, far).wait_recv()
            t_copy(d, far, core).start()

        pl.when(far > 0)(passed)

    last = jnp.minimum(index, reach * plane)
    pl.when(last > 0)(lambda: pass_on(1))

    def step(t, carry):
        pl.when((t < last) & (t != place + 1))(lambda: pass_on(t + 1))
        block, d, far = where_is(t)
        with jax.named_scope("A_wait"):
            t_copy(d, far, 1 - core).wait_recv()
        with jax.named_scope("A_block"):
            attend(block, False)

        @pl.when(t == place + 1)
        def _():
            for d in range(2, reach + 1):
                relay(d)
            pl.when(t < last)(lambda: pass_on(t + 1))

        return carry

    lax.fori_loop(1, last + 1, step, 0)

    for h in range(heads):
        done = (acc[h] / total[h : h + 1, :]).astype(jnp.bfloat16)
        for part in range(2):
            halves[part, h * VALUE_ENTRIES : (h + 1) * VALUE_ENTRIES, :] = done[:, part * half : (part + 1) * half]
    swap = remote(halves.at[1 - core], full.at[core], x_send, x_recv, (index, 1 - core))
    swap.start()
    full[core] = halves[core]
    loads[10].wait()
    loads[11].wait()
    with jax.named_scope("A_swap"):
        remote(halves.at[core], full.at[1 - core], x_send, x_recv, (index, 1 - core)).wait_recv()
    width = proj.shape[1]
    tile = math.gcd(width, 512)
    attended = full[...].reshape(proj.shape[0], half).astype(jnp.float32).T.astype(jnp.bfloat16)

    def project(j, carry):
        columns = pl.ds(pl.multiple_of(j * tile, tile), tile)
        mix[:, columns] = jnp.dot(attended, proj[:, columns], preferred_element_type=jnp.float32)
        return carry

    with jax.named_scope("A_project"):
        lax.fori_loop(0, width // tile, project, 0)

    def settle(j, carry):
        some = pl.ds(pl.multiple_of(j * 16, 16), 16)
        branch = rms_scale(mix[some, :], mix_gain[...])
        kept = (residual[some, :].astype(jnp.float32) + branch).astype(jnp.bfloat16)
        middle[some, :] = kept
        normed[some, :] = rms_scale(kept.astype(jnp.float32), moe_gain[...]).astype(jnp.bfloat16)
        return carry

    with jax.named_scope("A_settle"):
        lax.fori_loop(0, half // 16, settle, 0, unroll=2)
    group_rows = grouped.shape[1]
    slots = groups * group_rows
    chooser[...] = jnp.where(
        lax.broadcasted_iota(jnp.int32, (slots, half), 0).astype(jnp.float32) == member, 1.0, 0.0
    ).astype(jnp.bfloat16)

    def ready(group):
        picks = chooser[pl.ds(pl.multiple_of(group * group_rows, group_rows), group_rows), :]
        for j in range(width // tile):
            columns = slice(j * tile, (j + 1) * tile)
            grouped[group, :, columns] = jnp.dot(
                picks, normed[:, columns], preferred_element_type=jnp.float32
            ).astype(jnp.bfloat16)

    for copy in loads[12:]:
        copy.wait()
    expert_stage(
        groups, plane, (index, core, level, place), ready, grouped, metas, returned,
        gate, up, down, *rest[:9], m_send, m_recv, *rest[9:],
    )

    spots = chooser[...].astype(jnp.float32).T.astype(jnp.bfloat16)
    for j in range(width // tile):
        columns = slice(j * tile, (j + 1) * tile)
        mixed = jnp.dot(
            spots, returned[:, :, columns].reshape(slots, tile), preferred_element_type=jnp.float32
        )
        out_ref[:, columns] = (middle[:, columns].astype(jnp.float32) + mixed).astype(jnp.bfloat16)
    swap.wait_send()
    for d in range(reach + 1):
        for far in range(0 if d else 1, plane):
            pl.when((level >= d) if far == 0 else wanted(d, far, False))(
                lambda d=d, far=far: t_copy(d, far, core).wait_send()
            )
            if far:
                pl.when(wanted(d, far, True))(lambda d=d, far=far: p_copy(d, far).wait_send())
    for d in range(1, reach + 1):
        pl.when(level + d < groups)(lambda d=d: z_copy(d).wait_send())
    for k in range(1, groups):
        m_copy(k).wait_send()


def layer(
    queries, latent, rope_key, wk, wv, proj, residual, expert_ids, doc_ids, route,
    mix_gain, moe_gain, gate, up, down, count,
):
    rows, rank = latent.shape
    half = rows // 2
    plane = count // GROUPS
    capacity = half // plane
    heads = wk.shape[1] // UNROTATED_DIM
    width = proj.shape[1]
    units = gate.shape[1]
    group_rows = half // 2
    cut = width // PARTS
    vmem = pl.BlockSpec(memory_space=pltpu.VMEM)
    hbm = pl.BlockSpec(memory_space=pltpu.HBM)
    dma = pltpu.SemaphoreType.DMA
    few, many = dma((GROUPS,)), dma((GROUPS * plane,))
    few_parts, many_parts = dma((GROUPS * PARTS,)), dma((GROUPS * PARTS * plane,))

    def held(*shape, dtype=jnp.bfloat16):
        return pltpu.VMEM(shape, dtype)

    loaded = (
        queries.T, latent, rope_key.T, wk, wv, proj, residual, expert_ids.T, doc_ids[None, :],
        route.T, mix_gain[None, :], moe_gain[None, :], gate, up, down,
    )
    table = held(GROUPS, 16, -(-group_rows // 128) * 128)
    block = held(GROUPS, PARTS, plane, capacity, cut)
    return pl.pallas_call(
        functools.partial(layer_kernel, GROUPS, plane, heads),
        out_shape=jax.ShapeDtypeStruct((half, width), jnp.bfloat16),
        in_specs=[hbm] * len(loaded),
        out_specs=vmem,
        scratch_shapes=[held(*array.shape, dtype=array.dtype) for array in loaded] + [
            held(half, width), held(GROUPS * group_rows, half), held(GROUPS, group_rows, width),
            held(count, 2, half + ROPE, rank),
            held(heads, HEAD_LANES, rows),
            held(heads * VALUE_ENTRIES, rank),
            held(heads, rows, dtype=jnp.float32),
            held(heads, rows, dtype=jnp.float32),
            held(heads, VALUE_ENTRIES, rows, dtype=jnp.float32),
            held(2, heads * VALUE_ENTRIES, half),
            held(2, heads * VALUE_ENTRIES, half),
            held(half, width, dtype=jnp.float32),
            held(half, width),
            held(GROUPS, group_rows, width), table, table,
            dma((len(loaded),)), few, few, many, many, many, many, dma, dma, few, few,
            held(GROUPS, group_rows, width),
            held(GROUPS, plane, capacity, width),
            held(GROUPS, 2, plane, capacity, width),
            held(2 * plane * capacity, units),
            held(GROUPS, PARTS, 2, plane, capacity, cut),
            block, block, block,
            held(GROUPS, PARTS, group_rows, cut),
            few, few, many, many, few, many, many,
            few_parts, few_parts, many_parts, many_parts, few_parts, few_parts, few_parts,
        ],
        compiler_params=pltpu.CompilerParams(
            collective_id=3, has_side_effects=True, vmem_limit_bytes=VMEM_GRANT
        ),
        name="layer",
    )(*loaded)


def local(
    residual,
    queries,
    latent,
    rope_key,
    doc_ids,
    latent_to_key,
    latent_to_value,
    out_proj,
    mix_gain,
    moe_gain,
    expert_ids,
    route_weight,
    gate_weight,
    up_weight,
    down_weight,
):
    return layer(
        queries, latent, rope_key, latent_to_key, latent_to_value, out_proj, residual,
        expert_ids, doc_ids, route_weight, mix_gain, moe_gain, gate_weight[0], up_weight[0],
        down_weight[0], lax.axis_size("sp"),
    )


def solution(mesh):
    in_specs = (
        P(("sp", "tp"), None),
        P("sp", "tp"),
        P("sp", None),
        P("sp", None),
        P("sp"),
        P(None, "tp"),
        P(None, "tp"),
        P(),
        P(),
        P(),
        P(("sp", "tp"), None),
        P(("sp", "tp"), None),
        P("sp", None, "tp"),
        P("sp", None, "tp"),
        P("sp", "tp", None),
    )
    out_specs = P(("sp", "tp"), None)
    return jax.shard_map(local, mesh=mesh, in_specs=in_specs, out_specs=out_specs, check_vma=False)
```

```python
import functools
import math

import jax
import jax.numpy as jnp
from jax import lax
from jax.experimental import pallas as pl
from jax.experimental.pallas import tpu as pltpu
from jax.sharding import PartitionSpec as P

UNROTATED_DIM = 64
ROPE = 32
VALUE_ENTRIES = 64
GROUPS = 4
HEAD_LANES = 128
VMEM_GRANT = 56 * 1024 * 1024
PARTS = 2
SOURCES = ((0, 1, 3, 2), (1, 0, 2, 3), (2, 0, 1, 3), (3, 0, 1, 2))
TARGETS = ((0, 1, 3, 2), (1, 2, 3, 0), (2, 1, 0, 3), (3, 0, 1, 2))
LOWER = ["out1 over0 ffn0 out2", "over1 ffn1 out3 over2", "ffn2 back2 over3 ffn3", "back3 back1 back0 comb2", "comb3 comb1 comb0"]
UPPER = ["out1 out2 over0 ffn0", "over1 ffn1 back1 out3", "over2 ffn2 back2 comb1", "over3 ffn3 back3 back0", "comb2 comb3 comb0"]
MESH = pl.DeviceIdType.MESH

rope_base = 10000.0
epsilon = 1e-06


def angles_of(first, count):
    half_width = ROPE // 2
    line = lax.broadcasted_iota(jnp.int32, (half_width, count), 0)
    frequency = jnp.zeros((half_width, count), jnp.float32)
    for i in range(half_width):
        frequency = jnp.where(line == i, rope_base ** (-i / half_width), frequency)
    positions = first + lax.broadcasted_iota(jnp.int32, (half_width, count), 1)
    angles = positions.astype(jnp.float32) * frequency
    return jnp.cos(angles), jnp.sin(angles)


def rms_scale(source, gain):
    return source * lax.rsqrt(jnp.mean(source * source, axis=-1, keepdims=True) + epsilon) * gain


def turn(pair, cosine, sine):
    half = ROPE // 2
    upper, lower = pair[:half].astype(jnp.float32), pair[half:].astype(jnp.float32)
    return jnp.concatenate(
        [upper * cosine - lower * sine, lower * cosine + upper * sine], axis=0
    ).astype(jnp.bfloat16)


def greet(groups, plane, meanwhile=None):
    index, core = lax.axis_index("sp"), lax.axis_index("tp")
    level, place = index // plane, lax.rem(index, plane)
    barrier = pltpu.get_barrier_semaphore()
    peers = [(lax.rem(level + d, groups) * plane + place, core) for d in range(1, groups)]
    peers += [(level * plane + lax.rem(place + d, plane), core) for d in range(1, plane)]
    peers += [(index, 1 - core)]
    for peer in peers:
        pl.semaphore_signal(barrier, inc=1, device_id=peer, device_id_type=MESH)
    if meanwhile is not None:
        meanwhile(index, core)
    pl.semaphore_wait(barrier, len(peers))
    return index, core, level, place


def remote(source, target, send_sem, recv_sem, peer):
    return pltpu.make_async_remote_copy(
        src_ref=source, dst_ref=target, send_sem=send_sem, recv_sem=recv_sem,
        device_id=peer, device_id_type=MESH,
    )


def level_order(groups):
    return sorted(range(groups), key=lambda d: min(d, groups - d))


def chosen(table, level, at):
    picked = 0
    for l, order in enumerate(table):
        picked = picked + jnp.where(level == l, order[at], 0)
    return picked


def expert_stage(
    groups, plane, where, ready, grouped, metas, out_ref,
    gate, up, down, landed, spread, arrived, hidden, partial, passed, mixed, back, merged,
    m_send, m_recv, z_send, z_recv, p_send, p_recv, own_sem, t_send, t_recv,
    x_send, x_recv, b_send, b_recv, keep_sem, r_send, r_recv,
):
    index, core, level, place = where
    started = []
    group_rows, width = grouped.shape[1:]
    capacity = spread.shape[2]
    slots = plane * capacity
    cut = width // PARTS
    source_of = [chosen(SOURCES, level, k) for k in range(groups)]
    target_of = [chosen(TARGETS, level, k) for k in range(groups)]

    def begin(copy):
        copy.start()
        started.append(copy)

    def z_copy(k):
        other = target_of[k]
        return remote(
            grouped.at[other], landed.at[level], z_send.at[k], z_recv.at[level],
            (other * plane + place, core),
        )

    def out_copies(k):
        copies = []
        for far in range(plane - 1, 0, -1):
            to = lax.rem(place + far, plane)
            copies.append(remote(
                spread.at[k, to], arrived.at[k, core, place],
                p_send.at[k * plane + far], p_recv.at[k * plane + place],
                (level * plane + to, core),
            ))
        return copies

    def own_copy(k):
        return pltpu.make_async_copy(
            spread.at[k, place], arrived.at[k, core, place], own_sem.at[k]
        )

    def send_out(k):
        source = source_of[k]
        if k == 0:
            rows = grouped[level]
        else:
            peer = (source * plane + place, core)
            remote(metas.at[source], metas.at[source], m_send.at[k], m_recv.at[source], peer).wait_recv()
            remote(grouped.at[source], landed.at[source], z_send.at[k], z_recv.at[source], peer).wait_recv()
            rows = landed[source]
        info = metas[source][:, :group_rows].astype(jnp.float32)
        slot = lax.broadcasted_iota(jnp.int32, (slots, group_rows), 0).astype(jnp.float32)
        chooser = jnp.where((slot == info[0:1]) | (slot == info[1:2]), 1.0, 0.0)
        picked = jnp.dot(chooser.astype(jnp.bfloat16), rows, preferred_element_type=jnp.float32)
        for e in range(plane):
            spread[k, e] = picked[e * capacity : (e + 1) * capacity].astype(jnp.bfloat16)
        for copy in out_copies(k):
            copy.start()
        own_copy(k).start()

    def hand_over(k):
        for far in range(plane):
            origin = lax.rem(place + plane - far, plane)
            if far:
                remote(
                    spread.at[k, origin], arrived.at[k, core, origin],
                    p_send.at[k * plane + far], p_recv.at[k * plane + origin],
                    (level * plane + origin, core),
                ).wait_recv()
            else:
                own_copy(k).wait()
            begin(remote(
                arrived.at[k, core, origin], arrived.at[k, core, origin],
                t_send.at[k * plane + far], t_recv.at[k * plane + origin], (index, 1 - core),
            ))

    def experts(k):
        for origin in range(plane):
            remote(
                arrived.at[k, 1 - core, origin], arrived.at[k, 1 - core, origin],
                t_send.at[k * plane], t_recv.at[k * plane + origin], (index, 1 - core),
            ).wait_recv()
        units = gate.shape[1]
        unit_tile = math.gcd(units, 256)
        tile = math.gcd(cut, 256)

        def hide(j, carry):
            columns = pl.ds(pl.multiple_of(j * unit_tile, unit_tile), unit_tile)
            rows = arrived[k].reshape(2 * slots, width)
            gated = jnp.dot(rows, gate[:, columns], preferred_element_type=jnp.float32)
            raised = jnp.dot(rows, up[:, columns], preferred_element_type=jnp.float32)
            hidden[:, columns] = (gated / (1.0 + jnp.exp(-gated)) * raised).astype(jnp.bfloat16)
            return carry

        with jax.named_scope(f"E_hide{k}"):
            lax.fori_loop(0, units // unit_tile, hide, 0)
        for part in range(PARTS):

            def lower(j, carry, part=part):
                offset = pl.multiple_of(j * tile, tile)
                columns = pl.ds(pl.multiple_of(part * cut + offset, tile), tile)
                piece = jnp.dot(hidden[...], down[:, columns], preferred_element_type=jnp.float32)
                partial[k, part, :, :, :, pl.ds(offset, tile)] = piece.reshape(
                    2, plane, capacity, tile
                ).astype(jnp.bfloat16)
                return carry

            with jax.named_scope(f"E_lower{k}"):
                lax.fori_loop(0, cut // tile, lower, 0)
            at = k * PARTS + part
            begin(remote(
                partial.at[k, part, 1 - core], passed.at[k, part], x_send.at[at], x_recv.at[at],
                (index, 1 - core),
            ))

    def keep_copy(k, part):
        return pltpu.make_async_copy(
            mixed.at[k, part, place], back.at[k, part, place], keep_sem.at[k * PARTS + part]
        )

    def send_back(k):
        for part in range(PARTS):
            at = k * PARTS + part
            remote(
                partial.at[k, part, core], passed.at[k, part], x_send.at[at], x_recv.at[at],
                (index, 1 - core),
            ).wait_recv()
            for e in range(plane):
                mixed[k, part, e] = (
                    partial[k, part, core, e].astype(jnp.float32) + passed[k, part, e].astype(jnp.float32)
                ).astype(jnp.bfloat16)
            for far in range(plane - 1, 0, -1):
                to = lax.rem(place + far, plane)
                begin(remote(
                    mixed.at[k, part, to], back.at[k, part, place],
                    b_send.at[at * plane + far], b_recv.at[at * plane + place],
                    (level * plane + to, core),
                ))
            keep_copy(k, part).start()

    def combine(k):
        source = source_of[k]
        info = metas[source][:, :group_rows].astype(jnp.float32)
        slot = lax.broadcasted_iota(jnp.int32, (slots, group_rows), 0).astype(jnp.float32)
        hit_first, hit_second = slot == info[0:1], slot == info[1:2]
        for part in range(PARTS):
            at = k * PARTS + part
            for far in range(1, plane):
                origin = lax.rem(place + plane - far, plane)
                remote(
                    mixed.at[k, part, origin], back.at[k, part, origin],
                    b_send.at[at * plane + far], b_recv.at[at * plane + origin],
                    (level * plane + origin, core),
                ).wait_recv()
            keep_copy(k, part).wait()
            returned = back[k, part].reshape(slots, cut)
            result = 0.0
            for term in range(2):
                share = jnp.where(hit_first, info[2 + term : 3 + term], 0.0) + jnp.where(
                    hit_second, info[4 + term : 5 + term], 0.0
                )
                result = result + lax.dot_general(
                    share.astype(jnp.bfloat16), returned, (((0,), (0,)), ((), ())),
                    preferred_element_type=jnp.float32,
                )
            columns = slice(part * cut, (part + 1) * cut)
            if k == 0:
                out_ref[level, :, columns] = result.astype(jnp.bfloat16)
            else:
                merged[k, part] = result.astype(jnp.bfloat16)
                begin(remote(
                    merged.at[k, part], out_ref.at[level, :, columns],
                    r_send.at[at], r_recv.at[level * PARTS + part], (source * plane + place, core),
                ))

    steps = dict(out=send_out, over=hand_over, ffn=experts, back=send_back, comb=combine)

    def staged(name):
        with jax.named_scope("E_" + name):
            steps[name[:-1]](int(name[-1]))

    def finish(order):
        for name in " ".join(order).split():
            staged(name)
        with jax.named_scope("E_rest"):
            for k in range(1, groups):
                other = source_of[k]
                for part in range(PARTS):
                    at = k * PARTS + part
                    remote(
                        merged.at[k, part], out_ref.at[other, :, part * cut : (part + 1) * cut],
                        r_send.at[at], r_recv.at[other * PARTS + part], (other * plane + place, core),
                    ).wait_recv()
        for copy in started:
            copy.wait_send()
        started.clear()

    for k in (1, 0, 2, 3):
        ready(target_of[k])
        if k:
            z_copy(k).start()
        else:
            staged("out0")
    pl.when(level < groups // 2)(lambda: finish(LOWER))
    pl.when(level >= groups // 2)(lambda: finish(UPPER))
    for k in range(groups):
        if k:
            z_copy(k).wait_send()
        for copy in out_copies(k):
            copy.wait_send()


def assign(groups, plane, expert_ids, route, meta_ref):
    row_count = expert_ids.shape[1]
    count = groups * plane
    capacity = row_count // plane
    group_rows = row_count // 2
    ids = expert_ids.astype(jnp.float32)
    first, second = ids[0:1], ids[1:2]
    bins = -(-(count + groups) // 16) * 16
    line = lax.broadcasted_iota(jnp.int32, (bins, row_count), 0).astype(jnp.float32)
    group = jnp.zeros_like(first)
    for g in range(1, groups):
        group = group + jnp.where(first >= g * plane, 1.0, 0.0)
    hit_first, hit_second = line == first, line == second
    hit_group = line == group + count
    named = jnp.where(hit_first | hit_second | hit_group, 1.0, 0.0).astype(jnp.bfloat16)
    square = (row_count, row_count)
    before = jnp.where(
        lax.broadcasted_iota(jnp.int32, square, 0) < lax.broadcasted_iota(jnp.int32, square, 1), 1.0, 0.0
    ).astype(jnp.bfloat16)
    earlier = jnp.dot(named, before, preferred_element_type=jnp.float32)

    def rank_of(hit):
        return jnp.sum(jnp.where(hit, earlier, 0.0), axis=0, keepdims=True)

    member = group * group_rows + rank_of(hit_group)
    base = group * plane
    fields = [
        (first - base) * capacity + rank_of(hit_first) + 1.0,
        (second - base) * capacity + rank_of(hit_second) + 1.0,
    ]
    for term in range(2):
        weight = route[term : term + 1]
        coarse = weight.astype(jnp.bfloat16).astype(jnp.float32)
        fields += [coarse, weight - coarse]
    line = lax.broadcasted_iota(jnp.int32, (16, row_count), 0)
    table = jnp.zeros((16, row_count), jnp.float32)
    for at, field in enumerate(fields):
        table = jnp.where(line == at, field, table)
    table = table.astype(jnp.bfloat16)
    lanes = meta_ref.shape[2]
    spot = lax.broadcasted_iota(jnp.int32, (lanes, row_count), 0).astype(jnp.float32)
    free = jnp.where(lax.broadcasted_iota(jnp.int32, (16, lanes), 0) < 2, 1.0, 0.0)
    for g in range(groups):
        taken = (spot + g * group_rows == member) & (spot < group_rows)
        info = lax.dot_general(
            table, jnp.where(taken, 1.0, 0.0).astype(jnp.bfloat16), (((1,), (1,)), ((), ())),
            preferred_element_type=jnp.float32,
        )
        meta_ref[g] = (info - free).astype(jnp.bfloat16)
    return member


def layer_kernel(
    groups, plane, heads,
    query_hbm, latent_hbm, rope_hbm, wk_hbm, wv_hbm, proj_hbm, residual_hbm,
    ids_hbm, docs_hbm, route_hbm, mix_gain_hbm, moe_gain_hbm, gate_hbm, up_hbm, down_hbm,
    out_ref,
    query, latent, rope, wk, wv, proj, residual, expert_ids, doc_ids, route, mix_gain, moe_gain,
    gate, up, down, middle, chooser, returned,
    packs, turned, wv_turned, high, total, acc, halves, full, mix, normed, grouped, meta, metas,
    load_sem, z_send, z_recv, p_send, p_recv, t_send, t_recv, x_send, x_recv, m_send, m_recv, *rest,
):
    loads = [
        pltpu.make_async_copy(source, target, load_sem.at[i])
        for i, (source, target) in enumerate([
            (latent_hbm, latent), (rope_hbm, rope), (docs_hbm, doc_ids), (query_hbm, query),
            (wk_hbm, wk), (wv_hbm, wv), (ids_hbm, expert_ids), (route_hbm, route),
            (mix_gain_hbm, mix_gain), (moe_gain_hbm, moe_gain), (residual_hbm, residual),
            (proj_hbm, proj), (gate_hbm, gate), (up_hbm, up), (down_hbm, down),
        ])
    ]
    for copy in loads:
        copy.start()
    rows = latent.shape[0]
    half = rows // 2
    per_head = UNROTATED_DIM + ROPE
    cosine, sine = angles_of(lax.axis_index("sp") * rows, rows)

    def pack(index, core):
        for copy in loads[:3]:
            copy.wait()
        docs = doc_ids[...].astype(jnp.float32)
        key = turn(rope[...], cosine, sine)
        for part in range(2):
            span = slice(part * half, (part + 1) * half)
            packs[index, part, :half, :] = latent[span, :]
            line = lax.broadcasted_iota(jnp.int32, (ROPE, half), 0)
            ids = jnp.where(line == 0, jnp.broadcast_to(docs[:, span], (ROPE, half)), 0.0)
            packs[index, part, half:, :half] = key[:, span]
            packs[index, part, half:, half : 2 * half] = ids.astype(jnp.bfloat16)

    with jax.named_scope("A_greet"):
        index, core, level, place = greet(groups, plane, pack)
    reach = groups // 2

    def z_copy(d):
        return remote(
            packs.at[index, core], packs.at[index, core], z_send.at[d], z_recv.at[d],
            (lax.rem(level + d, groups) * plane + place, core),
        )

    def z_arrival(d):
        block = lax.rem(level + groups - d, groups) * plane + place
        return remote(
            packs.at[block, core], packs.at[block, core], z_send.at[d], z_recv.at[d],
            (block, core),
        )

    def p_copy(d, far):
        block = lax.rem(level + groups - d, groups) * plane + place
        return remote(
            packs.at[block, core], packs.at[block, core], p_send.at[d * plane + far],
            p_recv.at[d * plane + far],
            (level * plane + lax.rem(place + far, plane), core),
        )

    def p_arrival(d, far):
        origin = lax.rem(place + plane - far, plane)
        block = lax.rem(level + groups - d, groups) * plane + origin
        return remote(
            packs.at[block, core], packs.at[block, core], p_send.at[d * plane + far],
            p_recv.at[d * plane + far], (level * plane + origin, core),
        )

    def t_copy(d, far, part):
        origin = lax.rem(place + plane - far, plane)
        block = lax.rem(level + groups - d, groups) * plane + origin
        return remote(
            packs.at[block, part], packs.at[block, part], t_send.at[d * plane + far],
            t_recv.at[d * plane + far], (index, 1 - core),
        )

    odd = lax.rem(place, 2) == 1
    spans = [jnp.where(odd, plane - far, far) for far in range(1, plane)]

    def wanted(d, far, sender):
        ahead = lax.rem(place + far, plane) > place if sender else place >= far
        live = level >= d
        if d == 0:
            return live & ahead
        if d == reach:
            return live & jnp.logical_not(ahead)
        return live

    for d in range(1, reach + 1):
        pl.when(level + d < groups)(lambda d=d: z_copy(d).start())
    for far in spans:
        pl.when(wanted(0, far, True))(lambda far=far: p_copy(0, far).start())

    for copy in loads[3:10]:
        copy.wait()
    docs = doc_ids[...].astype(jnp.float32)
    with jax.named_scope("A_assign"):
        member = assign(groups, plane, expert_ids[...], route[...], meta)
    metas[level] = meta[level]

    def m_copy(k):
        other = chosen(TARGETS, level, k)
        return remote(
            meta.at[other], metas.at[level], m_send.at[k], m_recv.at[level],
            (other * plane + place, core),
        )

    for k in range(1, groups):
        m_copy(k).start()
    blank = jnp.zeros((HEAD_LANES - per_head, rows), jnp.bfloat16)
    for h in range(heads):
        own = query[h * per_head : (h + 1) * per_head, :]
        plain, moved = own[:UNROTATED_DIM], turn(own[UNROTATED_DIM:], cosine, sine)
        parts = [plain, moved, blank] if h % 2 == 0 else [moved, blank, plain]
        turned[h] = jnp.concatenate(parts, axis=0)
    wv_turned[...] = wv[...].astype(jnp.float32).T.astype(jnp.bfloat16)
    power = per_head ** (-0.5) * math.log2(math.e)

    def attend(block, first):
        source = jnp.concatenate([packs[block, part, :half, :] for part in range(2)], axis=0)
        tail = jnp.concatenate(
            [
                jnp.concatenate([packs[block, part, half:, :half] for part in range(2)], axis=1),
                jnp.concatenate(
                    [packs[block, part, half : half + 16, half : 2 * half] for part in range(2)], axis=1
                ),
            ],
            axis=0,
        )
        shape = (ROPE + 16, 3 * HEAD_LANES)
        line = lax.broadcasted_iota(jnp.int32, shape, 0)
        lane = lax.broadcasted_iota(jnp.int32, shape, 1)
        keyed = (line < ROPE) & ((lane == line + UNROTATED_DIM) | (lane == line + 2 * HEAD_LANES))
        named = (line == ROPE) & (lane >= HEAD_LANES) & (lane < 2 * HEAD_LANES)
        chooser = jnp.where(keyed | named, 1.0, 0.0).astype(jnp.bfloat16)
        extra = lax.dot_general(
            tail, chooser, (((0,), (0,)), ((), ())), preferred_element_type=jnp.float32
        )
        extras = [
            extra[:, :HEAD_LANES].astype(jnp.bfloat16), extra[:, 2 * HEAD_LANES :].astype(jnp.bfloat16)
        ]
        theirs = extra[:, HEAD_LANES : 2 * HEAD_LANES]
        theirs = jnp.concatenate([theirs] * (rows // HEAD_LANES), axis=1)
        live = theirs == docs
        if first:
            live = live & (
                lax.broadcasted_iota(jnp.int32, (rows, rows), 0)
                <= lax.broadcasted_iota(jnp.int32, (rows, rows), 1)
            )
        bias = jnp.where(live, 0.0, -1e30)
        keys = jnp.dot(source, wk[...], preferred_element_type=jnp.float32).astype(jnp.bfloat16)
        values = lax.dot_general(
            wv_turned[...], source, (((1,), (1,)), ((), ())), preferred_element_type=jnp.float32
        ).astype(jnp.bfloat16)
        side = lax.broadcasted_iota(jnp.int32, (rows, HEAD_LANES), 1) < UNROTATED_DIM
        for h in range(heads):
            low = h // 2 * HEAD_LANES
            pair = keys[:, low : low + HEAD_LANES]
            key = jnp.where(side, pair, extras[0]) if h % 2 == 0 else jnp.where(side, extras[1], pair)
            scores = jnp.dot(key, turned[h], preferred_element_type=jnp.float32) + bias
            top = jnp.max(scores, axis=0, keepdims=True)
            if not first:
                old = high[h : h + 1, :]
                top = jnp.maximum(old, top)
            weights = jnp.exp2((scores - top) * power)
            mass = jnp.sum(weights, axis=0, keepdims=True)
            mixed = jnp.dot(
                values[h * VALUE_ENTRIES : (h + 1) * VALUE_ENTRIES], weights.astype(jnp.bfloat16),
                preferred_element_type=jnp.float32,
            )
            high[h : h + 1, :] = top
            if first:
                total[h : h + 1, :] = mass
                acc[h] = mixed
            else:
                factor = jnp.exp2((old - top) * power)
                total[h : h + 1, :] = total[h : h + 1, :] * factor + mass
                acc[h] = acc[h] * factor + mixed

    with jax.named_scope("A_own"):
        attend(index, True)

    def relay(d):
        def arrived():
            with jax.named_scope(f"A_z{d}"):
                z_arrival(d).wait_recv()
            t_copy(d, 0, core).start()

        pl.when(level >= d)(arrived)
        for far in spans:
            pl.when(wanted(d, far, True))(lambda far=far: p_copy(d, far).start())

    relay(1)

    def where_is(t):
        below = t > place
        turn_at = jnp.where(below, t - place - 1, 0)
        d = jnp.where(below, 1 + turn_at // plane, 0)
        at = lax.rem(turn_at, plane)
        far = jnp.where(d == reach, place + at, at)
        far = jnp.where(at == 0, 0, jnp.where(odd, far, plane - at))
        far = jnp.where(below, far, t)
        block = (level - d) * plane + lax.rem(place + plane - far, plane)
        return block, d, far

    def pass_on(t):
        block, d, far = where_is(t)

        def passed():
            with jax.named_scope("A_pass"):
                p_arrival(d, far).wait_recv()
            t_copy(d, far, core).start()

        pl.when(far > 0)(passed)

    last = jnp.minimum(index, reach * plane)
    pl.when(last > 0)(lambda: pass_on(1))

    def step(t, carry):
        pl.when((t < last) & (t != place + 1))(lambda: pass_on(t + 1))
        block, d, far = where_is(t)
        with jax.named_scope("A_wait"):
            t_copy(d, far, 1 - core).wait_recv()
        with jax.named_scope("A_block"):
            attend(block, False)

        @pl.when(t == place + 1)
        def _():
            for d in range(2, reach + 1):
                relay(d)
            pl.when(t < last)(lambda: pass_on(t + 1))

        return carry

    lax.fori_loop(1, last + 1, step, 0)

    for h in range(heads):
        done = (acc[h] / total[h : h + 1, :]).astype(jnp.bfloat16)
        for part in range(2):
            halves[part, h * VALUE_ENTRIES : (h + 1) * VALUE_ENTRIES, :] = done[:, part * half : (part + 1) * half]
    swap = remote(halves.at[1 - core], full.at[core], x_send, x_recv, (index, 1 - core))
    swap.start()
    full[core] = halves[core]
    loads[10].wait()
    loads[11].wait()
    with jax.named_scope("A_swap"):
        remote(halves.at[core], full.at[1 - core], x_send, x_recv, (index, 1 - core)).wait_recv()
    width = proj.shape[1]
    tile = math.gcd(width, 512)
    attended = full[...].reshape(proj.shape[0], half).astype(jnp.float32).T.astype(jnp.bfloat16)

    def project(j, carry):
        columns = pl.ds(pl.multiple_of(j * tile, tile), tile)
        mix[:, columns] = jnp.dot(attended, proj[:, columns], preferred_element_type=jnp.float32)
        return carry

    with jax.named_scope("A_project"):
        lax.fori_loop(0, width // tile, project, 0)

    def settle(j, carry):
        some = pl.ds(pl.multiple_of(j * 16, 16), 16)
        branch = rms_scale(mix[some, :], mix_gain[...])
        kept = (residual[some, :].astype(jnp.float32) + branch).astype(jnp.bfloat16)
        middle[some, :] = kept
        normed[some, :] = rms_scale(kept.astype(jnp.float32), moe_gain[...]).astype(jnp.bfloat16)
        return carry

    with jax.named_scope("A_settle"):
        lax.fori_loop(0, half // 16, settle, 0, unroll=2)
    group_rows = grouped.shape[1]
    slots = groups * group_rows
    chooser[...] = jnp.where(
        lax.broadcasted_iota(jnp.int32, (slots, half), 0).astype(jnp.float32) == member, 1.0, 0.0
    ).astype(jnp.bfloat16)

    def ready(group):
        picks = chooser[pl.ds(pl.multiple_of(group * group_rows, group_rows), group_rows), :]
        for j in range(width // tile):
            columns = slice(j * tile, (j + 1) * tile)
            grouped[group, :, columns] = jnp.dot(
                picks, normed[:, columns], preferred_element_type=jnp.float32
            ).astype(jnp.bfloat16)

    for copy in loads[12:]:
        copy.wait()
    expert_stage(
        groups, plane, (index, core, level, place), ready, grouped, metas, returned,
        gate, up, down, *rest[:9], m_send, m_recv, *rest[9:],
    )

    spots = chooser[...].astype(jnp.float32).T.astype(jnp.bfloat16)
    for j in range(width // tile):
        columns = slice(j * tile, (j + 1) * tile)
        mixed = jnp.dot(
            spots, returned[:, :, columns].reshape(slots, tile), preferred_element_type=jnp.float32
        )
        out_ref[:, columns] = (middle[:, columns].astype(jnp.float32) + mixed).astype(jnp.bfloat16)
    swap.wait_send()
    for d in range(reach + 1):
        for far in range(0 if d else 1, plane):
            pl.when((level >= d) if far == 0 else wanted(d, far, False))(
                lambda d=d, far=far: t_copy(d, far, core).wait_send()
            )
            if far:
                pl.when(wanted(d, far, True))(lambda d=d, far=far: p_copy(d, far).wait_send())
    for d in range(1, reach + 1):
        pl.when(level + d < groups)(lambda d=d: z_copy(d).wait_send())
    for k in range(1, groups):
        m_copy(k).wait_send()


def layer(
    queries, latent, rope_key, wk, wv, proj, residual, expert_ids, doc_ids, route,
    mix_gain, moe_gain, gate, up, down, count,
):
    rows, rank = latent.shape
    half = rows // 2
    plane = count // GROUPS
    capacity = half // plane
    heads = wk.shape[1] // UNROTATED_DIM
    width = proj.shape[1]
    units = gate.shape[1]
    group_rows = half // 2
    cut = width // PARTS
    vmem = pl.BlockSpec(memory_space=pltpu.VMEM)
    hbm = pl.BlockSpec(memory_space=pltpu.HBM)
    dma = pltpu.SemaphoreType.DMA
    few, many = dma((GROUPS,)), dma((GROUPS * plane,))
    few_parts, many_parts = dma((GROUPS * PARTS,)), dma((GROUPS * PARTS * plane,))

    def held(*shape, dtype=jnp.bfloat16):
        return pltpu.VMEM(shape, dtype)

    loaded = (
        queries.T, latent, rope_key.T, wk, wv, proj, residual, expert_ids.T, doc_ids[None, :],
        route.T, mix_gain[None, :], moe_gain[None, :], gate, up, down,
    )
    table = held(GROUPS, 16, -(-group_rows // 128) * 128)
    block = held(GROUPS, PARTS, plane, capacity, cut)
    return pl.pallas_call(
        functools.partial(layer_kernel, GROUPS, plane, heads),
        out_shape=jax.ShapeDtypeStruct((half, width), jnp.bfloat16),
        in_specs=[hbm] * len(loaded),
        out_specs=vmem,
        scratch_shapes=[held(*array.shape, dtype=array.dtype) for array in loaded] + [
            held(half, width), held(GROUPS * group_rows, half), held(GROUPS, group_rows, width),
            held(count, 2, half + ROPE, rank),
            held(heads, HEAD_LANES, rows),
            held(heads * VALUE_ENTRIES, rank),
            held(heads, rows, dtype=jnp.float32),
            held(heads, rows, dtype=jnp.float32),
            held(heads, VALUE_ENTRIES, rows, dtype=jnp.float32),
            held(2, heads * VALUE_ENTRIES, half),
            held(2, heads * VALUE_ENTRIES, half),
            held(half, width, dtype=jnp.float32),
            held(half, width),
            held(GROUPS, group_rows, width), table, table,
            dma((len(loaded),)), few, few, many, many, many, many, dma, dma, few, few,
            held(GROUPS, group_rows, width),
            held(GROUPS, plane, capacity, width),
            held(GROUPS, 2, plane, capacity, width),
            held(2 * plane * capacity, units),
            held(GROUPS, PARTS, 2, plane, capacity, cut),
            block, block, block,
            held(GROUPS, PARTS, group_rows, cut),
            few, few, many, many, few, many, many,
            few_parts, few_parts, many_parts, many_parts, few_parts, few_parts, few_parts,
        ],
        compiler_params=pltpu.CompilerParams(
            collective_id=3, has_side_effects=True, vmem_limit_bytes=VMEM_GRANT
        ),
        name="layer",
    )(*loaded)


def local(
    residual,
    queries,
    latent,
    rope_key,
    doc_ids,
    latent_to_key,
    latent_to_value,
    out_proj,
    mix_gain,
    moe_gain,
    expert_ids,
    route_weight,
    gate_weight,
    up_weight,
    down_weight,
):
    return layer(
        queries, latent, rope_key, latent_to_key, latent_to_value, out_proj, residual,
        expert_ids, doc_ids, route_weight, mix_gain, moe_gain, gate_weight[0], up_weight[0],
        down_weight[0], lax.axis_size("sp"),
    )


def solution(mesh):
    in_specs = (
        P(("sp", "tp"), None),
        P("sp", "tp"),
        P("sp", None),
        P("sp", None),
        P("sp"),
        P(None, "tp"),
        P(None, "tp"),
        P(),
        P(),
        P(),
        P(("sp", "tp"), None),
        P(("sp", "tp"), None),
        P("sp", None, "tp"),
        P("sp", None, "tp"),
        P("sp", "tp", None),
    )
    out_specs = P(("sp", "tp"), None)
    return jax.shard_map(local, mesh=mesh, in_specs=in_specs, out_specs=out_specs, check_vma=False)
```

```python
import functools
import math

import jax
import jax.numpy as jnp
from jax import lax
from jax.experimental import pallas as pl
from jax.experimental.pallas import tpu as pltpu
from jax.sharding import PartitionSpec as P

UNROTATED_DIM = 64
ROPE = 32
VALUE_ENTRIES = 64
GROUPS = 4
HEAD_LANES = 128
VMEM_GRANT = 56 * 1024 * 1024
PARTS = 2
SOURCES = ((0, 1, 3, 2), (1, 0, 2, 3), (2, 0, 1, 3), (3, 0, 1, 2))
TARGETS = ((0, 1, 3, 2), (1, 2, 3, 0), (2, 1, 0, 3), (3, 0, 1, 2))
LOWEST = ["out1 over0 ffn0 out2", "over1 ffn1 out3 over2", "ffn2 back2 over3 ffn3", "comb2 back3 back1 back0", "comb3 comb1 comb0"]
LOWER = ["out1 over0 ffn0 over1", "back0 ffn1 out2 out3", "over2 ffn2 back2 over3", "ffn3 comb2 back3 back1", "comb3 comb1 comb0"]
UPPER = ["out1 out2 over0 ffn0", "over1 ffn1 back1 out3", "over2 ffn2 back2 comb1", "over3 ffn3 back3 back0", "comb2 comb3 comb0"]
MESH = pl.DeviceIdType.MESH

rope_base = 10000.0
epsilon = 1e-06


def angles_of(first, count):
    half_width = ROPE // 2
    line = lax.broadcasted_iota(jnp.int32, (half_width, count), 0)
    frequency = jnp.zeros((half_width, count), jnp.float32)
    for i in range(half_width):
        frequency = jnp.where(line == i, rope_base ** (-i / half_width), frequency)
    positions = first + lax.broadcasted_iota(jnp.int32, (half_width, count), 1)
    angles = positions.astype(jnp.float32) * frequency
    return jnp.cos(angles), jnp.sin(angles)


def rms_scale(source, gain):
    return source * lax.rsqrt(jnp.mean(source * source, axis=-1, keepdims=True) + epsilon) * gain


def turn(pair, cosine, sine):
    half = ROPE // 2
    upper, lower = pair[:half].astype(jnp.float32), pair[half:].astype(jnp.float32)
    return jnp.concatenate(
        [upper * cosine - lower * sine, lower * cosine + upper * sine], axis=0
    ).astype(jnp.bfloat16)


def greet(groups, plane, meanwhile=None):
    index, core = lax.axis_index("sp"), lax.axis_index("tp")
    level, place = index // plane, lax.rem(index, plane)
    barrier = pltpu.get_barrier_semaphore()
    peers = [(lax.rem(level + d, groups) * plane + place, core) for d in range(1, groups)]
    peers += [(level * plane + lax.rem(place + d, plane), core) for d in range(1, plane)]
    peers += [(index, 1 - core)]
    for peer in peers:
        pl.semaphore_signal(barrier, inc=1, device_id=peer, device_id_type=MESH)
    if meanwhile is not None:
        meanwhile(index, core)
    pl.semaphore_wait(barrier, len(peers))
    return index, core, level, place


def remote(source, target, send_sem, recv_sem, peer):
    return pltpu.make_async_remote_copy(
        src_ref=source, dst_ref=target, send_sem=send_sem, recv_sem=recv_sem,
        device_id=peer, device_id_type=MESH,
    )


def level_order(groups):
    return sorted(range(groups), key=lambda d: min(d, groups - d))


def chosen(table, level, at):
    picked = 0
    for l, order in enumerate(table):
        picked = picked + jnp.where(level == l, order[at], 0)
    return picked


def expert_stage(
    groups, plane, where, ready, settle_sends, conclude, grouped, metas, out_ref,
    gate, up, down, landed, spread, arrived, hidden, partial, passed, mixed, back, merged,
    m_send, m_recv, z_send, z_recv, p_send, p_recv, own_sem, t_send, t_recv,
    x_send, x_recv, b_send, b_recv, keep_sem, r_send, r_recv,
):
    index, core, level, place = where
    started = []
    group_rows, width = grouped.shape[1:]
    capacity = spread.shape[2]
    slots = plane * capacity
    cut = width // PARTS
    source_of = [chosen(SOURCES, level, k) for k in range(groups)]
    target_of = [chosen(TARGETS, level, k) for k in range(groups)]

    def begin(copy):
        copy.start()
        started.append(copy)

    def z_copy(k):
        other = target_of[k]
        return remote(
            grouped.at[other], landed.at[level], z_send.at[k], z_recv.at[level],
            (other * plane + place, core),
        )

    def out_copies(k):
        copies = []
        for far in range(plane - 1, 0, -1):
            to = lax.rem(place + far, plane)
            copies.append(remote(
                spread.at[k, to], arrived.at[k, core, place],
                p_send.at[k * plane + far], p_recv.at[k * plane + place],
                (level * plane + to, core),
            ))
        return copies

    def own_copy(k):
        return pltpu.make_async_copy(
            spread.at[k, place], arrived.at[k, core, place], own_sem.at[k]
        )

    def send_out(k):
        source = source_of[k]
        if k == 0:
            rows = grouped[level]
        else:
            peer = (source * plane + place, core)
            remote(metas.at[source], metas.at[source], m_send.at[k], m_recv.at[source], peer).wait_recv()
            remote(grouped.at[source], landed.at[source], z_send.at[k], z_recv.at[source], peer).wait_recv()
            rows = landed[source]
        info = metas[source][:, :group_rows].astype(jnp.float32)
        slot = lax.broadcasted_iota(jnp.int32, (slots, group_rows), 0).astype(jnp.float32)
        chooser = jnp.where((slot == info[0:1]) | (slot == info[1:2]), 1.0, 0.0)
        picked = jnp.dot(chooser.astype(jnp.bfloat16), rows, preferred_element_type=jnp.float32)
        for e in range(plane):
            spread[k, e] = picked[e * capacity : (e + 1) * capacity].astype(jnp.bfloat16)
        for copy in out_copies(k):
            copy.start()
        own_copy(k).start()

    def hand_over(k):
        for far in range(plane):
            origin = lax.rem(place + plane - far, plane)
            if far:
                remote(
                    spread.at[k, origin], arrived.at[k, core, origin],
                    p_send.at[k * plane + far], p_recv.at[k * plane + origin],
                    (level * plane + origin, core),
                ).wait_recv()
            else:
                own_copy(k).wait()
            begin(remote(
                arrived.at[k, core, origin], arrived.at[k, core, origin],
                t_send.at[k * plane + far], t_recv.at[k * plane + origin], (index, 1 - core),
            ))

    def experts(k):
        for origin in range(plane):
            remote(
                arrived.at[k, 1 - core, origin], arrived.at[k, 1 - core, origin],
                t_send.at[k * plane], t_recv.at[k * plane + origin], (index, 1 - core),
            ).wait_recv()
        units = gate.shape[1]
        unit_tile = math.gcd(units, 256)
        tile = math.gcd(cut, 256)

        def hide(j, carry):
            columns = pl.ds(pl.multiple_of(j * unit_tile, unit_tile), unit_tile)
            rows = arrived[k].reshape(2 * slots, width)
            gated = jnp.dot(rows, gate[:, columns], preferred_element_type=jnp.float32)
            raised = jnp.dot(rows, up[:, columns], preferred_element_type=jnp.float32)
            hidden[:, columns] = (gated / (1.0 + jnp.exp(-gated)) * raised).astype(jnp.bfloat16)
            return carry

        with jax.named_scope(f"E_hide{k}"):
            lax.fori_loop(0, units // unit_tile, hide, 0)
        for part in range(PARTS):

            def lower(j, carry, part=part):
                offset = pl.multiple_of(j * tile, tile)
                columns = pl.ds(pl.multiple_of(part * cut + offset, tile), tile)
                piece = jnp.dot(hidden[...], down[:, columns], preferred_element_type=jnp.float32)
                partial[k, part, :, :, :, pl.ds(offset, tile)] = piece.reshape(
                    2, plane, capacity, tile
                ).astype(jnp.bfloat16)
                return carry

            with jax.named_scope(f"E_lower{k}"):
                lax.fori_loop(0, cut // tile, lower, 0)
            at = k * PARTS + part
            begin(remote(
                partial.at[k, part, 1 - core], passed.at[k, part], x_send.at[at], x_recv.at[at],
                (index, 1 - core),
            ))

    def keep_copy(k, part):
        return pltpu.make_async_copy(
            mixed.at[k, part, place], back.at[k, part, place], keep_sem.at[k * PARTS + part]
        )

    def send_back(k):
        for part in range(PARTS):
            at = k * PARTS + part
            remote(
                partial.at[k, part, core], passed.at[k, part], x_send.at[at], x_recv.at[at],
                (index, 1 - core),
            ).wait_recv()
            for e in range(plane):
                mixed[k, part, e] = (
                    partial[k, part, core, e].astype(jnp.float32) + passed[k, part, e].astype(jnp.float32)
                ).astype(jnp.bfloat16)
            for far in range(plane - 1, 0, -1):
                to = lax.rem(place + far, plane)
                begin(remote(
                    mixed.at[k, part, to], back.at[k, part, place],
                    b_send.at[at * plane + far], b_recv.at[at * plane + place],
                    (level * plane + to, core),
                ))
            keep_copy(k, part).start()

    def combine(k):
        source = source_of[k]
        info = metas[source][:, :group_rows].astype(jnp.float32)
        slot = lax.broadcasted_iota(jnp.int32, (slots, group_rows), 0).astype(jnp.float32)
        hit_first, hit_second = slot == info[0:1], slot == info[1:2]
        for part in range(PARTS):
            at = k * PARTS + part
            for far in range(1, plane):
                origin = lax.rem(place + plane - far, plane)
                remote(
                    mixed.at[k, part, origin], back.at[k, part, origin],
                    b_send.at[at * plane + far], b_recv.at[at * plane + origin],
                    (level * plane + origin, core),
                ).wait_recv()
            keep_copy(k, part).wait()
            returned = back[k, part].reshape(slots, cut)
            result = 0.0
            for term in range(2):
                share = jnp.where(hit_first, info[2 + term : 3 + term], 0.0) + jnp.where(
                    hit_second, info[4 + term : 5 + term], 0.0
                )
                result = result + lax.dot_general(
                    share.astype(jnp.bfloat16), returned, (((0,), (0,)), ((), ())),
                    preferred_element_type=jnp.float32,
                )
            columns = slice(part * cut, (part + 1) * cut)
            if k == 0:
                out_ref[level, :, columns] = result.astype(jnp.bfloat16)
            else:
                merged[k, part] = result.astype(jnp.bfloat16)
                begin(remote(
                    merged.at[k, part], out_ref.at[level, :, columns],
                    r_send.at[at], r_recv.at[level * PARTS + part], (source * plane + place, core),
                ))

    steps = dict(out=send_out, over=hand_over, ffn=experts, back=send_back, comb=combine)

    def staged(name):
        with jax.named_scope("E_" + name):
            steps[name[:-1]](int(name[-1]))

    def finish(order):
        for name in " ".join(order).split():
            staged(name)
        for copy in started[: -2 * PARTS]:
            copy.wait_send()
        for k in range(groups):
            if k:
                z_copy(k).wait_send()
            for copy in out_copies(k):
                copy.wait_send()
        with jax.named_scope("E_rest"):
            for part in range(PARTS):
                for k in range(1, groups):
                    other = source_of[k]
                    remote(
                        merged.at[k, part], out_ref.at[other, :, part * cut : (part + 1) * cut],
                        r_send.at[k * PARTS + part], r_recv.at[other * PARTS + part],
                        (other * plane + place, core),
                    ).wait_recv()
                conclude(part)
        for copy in started[-2 * PARTS :]:
            copy.wait_send()
        started.clear()

    for k in (1, 0, 2, 3):
        ready(target_of[k])
        if k:
            z_copy(k).start()
        else:
            staged("out0")
    settle_sends()
    pl.when(level == 0)(lambda: finish(LOWEST))
    pl.when((level > 0) & (level < groups // 2))(lambda: finish(LOWER))
    pl.when(level >= groups // 2)(lambda: finish(UPPER))


def assign(groups, plane, expert_ids, route, meta_ref):
    row_count = expert_ids.shape[1]
    count = groups * plane
    capacity = row_count // plane
    group_rows = row_count // 2
    ids = expert_ids.astype(jnp.float32)
    first, second = ids[0:1], ids[1:2]
    bins = -(-(count + groups) // 16) * 16
    line = lax.broadcasted_iota(jnp.int32, (bins, row_count), 0).astype(jnp.float32)
    group = jnp.zeros_like(first)
    for g in range(1, groups):
        group = group + jnp.where(first >= g * plane, 1.0, 0.0)
    hit_first, hit_second = line == first, line == second
    hit_group = line == group + count
    named = jnp.where(hit_first | hit_second | hit_group, 1.0, 0.0).astype(jnp.bfloat16)
    square = (row_count, row_count)
    before = jnp.where(
        lax.broadcasted_iota(jnp.int32, square, 0) < lax.broadcasted_iota(jnp.int32, square, 1), 1.0, 0.0
    ).astype(jnp.bfloat16)
    earlier = jnp.dot(named, before, preferred_element_type=jnp.float32)

    def rank_of(hit):
        return jnp.sum(jnp.where(hit, earlier, 0.0), axis=0, keepdims=True)

    member = group * group_rows + rank_of(hit_group)
    base = group * plane
    fields = [
        (first - base) * capacity + rank_of(hit_first) + 1.0,
        (second - base) * capacity + rank_of(hit_second) + 1.0,
    ]
    for term in range(2):
        weight = route[term : term + 1]
        coarse = weight.astype(jnp.bfloat16).astype(jnp.float32)
        fields += [coarse, weight - coarse]
    line = lax.broadcasted_iota(jnp.int32, (16, row_count), 0)
    table = jnp.zeros((16, row_count), jnp.float32)
    for at, field in enumerate(fields):
        table = jnp.where(line == at, field, table)
    table = table.astype(jnp.bfloat16)
    lanes = meta_ref.shape[2]
    spot = lax.broadcasted_iota(jnp.int32, (lanes, row_count), 0).astype(jnp.float32)
    free = jnp.where(lax.broadcasted_iota(jnp.int32, (16, lanes), 0) < 2, 1.0, 0.0)
    for g in range(groups):
        taken = (spot + g * group_rows == member) & (spot < group_rows)
        info = lax.dot_general(
            table, jnp.where(taken, 1.0, 0.0).astype(jnp.bfloat16), (((1,), (1,)), ((), ())),
            preferred_element_type=jnp.float32,
        )
        meta_ref[g] = (info - free).astype(jnp.bfloat16)
    return member


def layer_kernel(
    groups, plane, heads,
    query_hbm, latent_hbm, rope_hbm, wk_hbm, wv_hbm, proj_hbm, residual_hbm,
    ids_hbm, docs_hbm, route_hbm, mix_gain_hbm, moe_gain_hbm, gate_hbm, up_hbm, down_hbm,
    out_ref,
    query, latent, rope, wk, wv, proj, residual, expert_ids, doc_ids, route, mix_gain, moe_gain,
    gate, up, down, middle, chooser, returned, spots, total_out,
    packs, turned, wv_turned, high, total, acc, halves, full, mix, normed, grouped, meta, metas,
    load_sem, o_sem, z_send, z_recv, p_send, p_recv, t_send, t_recv, x_send, x_recv, m_send, m_recv, *rest,
):
    loads = [
        pltpu.make_async_copy(source, target, load_sem.at[i])
        for i, (source, target) in enumerate([
            (latent_hbm, latent), (rope_hbm, rope), (docs_hbm, doc_ids), (query_hbm, query),
            (wk_hbm, wk), (wv_hbm, wv), (ids_hbm, expert_ids), (route_hbm, route),
            (mix_gain_hbm, mix_gain), (moe_gain_hbm, moe_gain), (residual_hbm, residual),
            (proj_hbm, proj), (gate_hbm, gate), (up_hbm, up), (down_hbm, down),
        ])
    ]
    for copy in loads:
        copy.start()
    rows = latent.shape[0]
    half = rows // 2
    per_head = UNROTATED_DIM + ROPE
    cosine, sine = angles_of(lax.axis_index("sp") * rows, rows)

    def pack(index, core):
        for copy in loads[:3]:
            copy.wait()
        docs = doc_ids[...].astype(jnp.float32)
        key = turn(rope[...], cosine, sine)
        for part in range(2):
            span = slice(part * half, (part + 1) * half)
            packs[index, part, :half, :] = latent[span, :]
            line = lax.broadcasted_iota(jnp.int32, (ROPE, half), 0)
            ids = jnp.where(line == 0, jnp.broadcast_to(docs[:, span], (ROPE, half)), 0.0)
            packs[index, part, half:, :half] = key[:, span]
            packs[index, part, half:, half : 2 * half] = ids.astype(jnp.bfloat16)

    with jax.named_scope("A_greet"):
        index, core, level, place = greet(groups, plane, pack)
    reach = groups // 2

    def z_copy(d):
        return remote(
            packs.at[index, core], packs.at[index, core], z_send.at[d], z_recv.at[d],
            (lax.rem(level + d, groups) * plane + place, core),
        )

    def z_arrival(d):
        block = lax.rem(level + groups - d, groups) * plane + place
        return remote(
            packs.at[block, core], packs.at[block, core], z_send.at[d], z_recv.at[d],
            (block, core),
        )

    def p_copy(d, far):
        block = lax.rem(level + groups - d, groups) * plane + place
        return remote(
            packs.at[block, core], packs.at[block, core], p_send.at[d * plane + far],
            p_recv.at[d * plane + far],
            (level * plane + lax.rem(place + far, plane), core),
        )

    def p_arrival(d, far):
        origin = lax.rem(place + plane - far, plane)
        block = lax.rem(level + groups - d, groups) * plane + origin
        return remote(
            packs.at[block, core], packs.at[block, core], p_send.at[d * plane + far],
            p_recv.at[d * plane + far], (level * plane + origin, core),
        )

    def t_copy(d, far, part):
        origin = lax.rem(place + plane - far, plane)
        block = lax.rem(level + groups - d, groups) * plane + origin
        return remote(
            packs.at[block, part], packs.at[block, part], t_send.at[d * plane + far],
            t_recv.at[d * plane + far], (index, 1 - core),
        )

    odd = lax.rem(place, 2) == 1
    spans = [jnp.where(odd, plane - far, far) for far in range(1, plane)]

    def wanted(d, far, sender):
        ahead = lax.rem(place + far, plane) > place if sender else place >= far
        live = level >= d
        if d == 0:
            return live & ahead
        if d == reach:
            return live & jnp.logical_not(ahead)
        return live

    for d in range(1, reach + 1):
        pl.when(level + d < groups)(lambda d=d: z_copy(d).start())
    for far in spans:
        pl.when(wanted(0, far, True))(lambda far=far: p_copy(0, far).start())

    for copy in loads[3:10]:
        copy.wait()
    docs = doc_ids[...].astype(jnp.float32)
    with jax.named_scope("A_assign"):
        member = assign(groups, plane, expert_ids[...], route[...], meta)
    metas[level] = meta[level]

    def m_copy(k):
        other = chosen(TARGETS, level, k)
        return remote(
            meta.at[other], metas.at[level], m_send.at[k], m_recv.at[level],
            (other * plane + place, core),
        )

    for k in range(1, groups):
        m_copy(k).start()
    blank = jnp.zeros((HEAD_LANES - per_head, rows), jnp.bfloat16)
    for h in range(heads):
        own = query[h * per_head : (h + 1) * per_head, :]
        plain, moved = own[:UNROTATED_DIM], turn(own[UNROTATED_DIM:], cosine, sine)
        parts = [plain, moved, blank] if h % 2 == 0 else [moved, blank, plain]
        turned[h] = jnp.concatenate(parts, axis=0)
    wv_turned[...] = wv[...].astype(jnp.float32).T.astype(jnp.bfloat16)
    power = per_head ** (-0.5) * math.log2(math.e)

    def attend(block, first):
        source = jnp.concatenate([packs[block, part, :half, :] for part in range(2)], axis=0)
        tail = jnp.concatenate(
            [
                jnp.concatenate([packs[block, part, half:, :half] for part in range(2)], axis=1),
                jnp.concatenate(
                    [packs[block, part, half : half + 16, half : 2 * half] for part in range(2)], axis=1
                ),
            ],
            axis=0,
        )
        shape = (ROPE + 16, 3 * HEAD_LANES)
        line = lax.broadcasted_iota(jnp.int32, shape, 0)
        lane = lax.broadcasted_iota(jnp.int32, shape, 1)
        keyed = (line < ROPE) & ((lane == line + UNROTATED_DIM) | (lane == line + 2 * HEAD_LANES))
        named = (line == ROPE) & (lane >= HEAD_LANES) & (lane < 2 * HEAD_LANES)
        chooser = jnp.where(keyed | named, 1.0, 0.0).astype(jnp.bfloat16)
        extra = lax.dot_general(
            tail, chooser, (((0,), (0,)), ((), ())), preferred_element_type=jnp.float32
        )
        extras = [
            extra[:, :HEAD_LANES].astype(jnp.bfloat16), extra[:, 2 * HEAD_LANES :].astype(jnp.bfloat16)
        ]
        theirs = extra[:, HEAD_LANES : 2 * HEAD_LANES]
        theirs = jnp.concatenate([theirs] * (rows // HEAD_LANES), axis=1)
        live = theirs == docs
        if first:
            live = live & (
                lax.broadcasted_iota(jnp.int32, (rows, rows), 0)
                <= lax.broadcasted_iota(jnp.int32, (rows, rows), 1)
            )
        bias = jnp.where(live, 0.0, -1e30)
        keys = jnp.dot(source, wk[...], preferred_element_type=jnp.float32).astype(jnp.bfloat16)
        values = lax.dot_general(
            wv_turned[...], source, (((1,), (1,)), ((), ())), preferred_element_type=jnp.float32
        ).astype(jnp.bfloat16)
        side = lax.broadcasted_iota(jnp.int32, (rows, HEAD_LANES), 1) < UNROTATED_DIM
        for h in range(heads):
            low = h // 2 * HEAD_LANES
            pair = keys[:, low : low + HEAD_LANES]
            key = jnp.where(side, pair, extras[0]) if h % 2 == 0 else jnp.where(side, extras[1], pair)
            scores = jnp.dot(key, turned[h], preferred_element_type=jnp.float32) + bias
            top = jnp.max(scores, axis=0, keepdims=True)
            if not first:
                old = high[h : h + 1, :]
                top = jnp.maximum(old, top)
            weights = jnp.exp2((scores - top) * power)
            mass = jnp.sum(weights, axis=0, keepdims=True)
            mixed = jnp.dot(
                values[h * VALUE_ENTRIES : (h + 1) * VALUE_ENTRIES], weights.astype(jnp.bfloat16),
                preferred_element_type=jnp.float32,
            )
            high[h : h + 1, :] = top
            if first:
                total[h : h + 1, :] = mass
                acc[h] = mixed
            else:
                factor = jnp.exp2((old - top) * power)
                total[h : h + 1, :] = total[h : h + 1, :] * factor + mass
                acc[h] = acc[h] * factor + mixed

    with jax.named_scope("A_own"):
        attend(index, True)

    def relay(d):
        def arrived():
            with jax.named_scope(f"A_z{d}"):
                z_arrival(d).wait_recv()
            t_copy(d, 0, core).start()

        pl.when(level >= d)(arrived)
        for far in spans:
            pl.when(wanted(d, far, True))(lambda far=far: p_copy(d, far).start())

    relay(1)

    def where_is(t):
        below = t > place
        turn_at = jnp.where(below, t - place - 1, 0)
        d = jnp.where(below, 1 + turn_at // plane, 0)
        at = lax.rem(turn_at, plane)
        far = jnp.where(d == reach, place + at, at)
        far = jnp.where(at == 0, 0, jnp.where(odd, far, plane - at))
        far = jnp.where(below, far, t)
        block = (level - d) * plane + lax.rem(place + plane - far, plane)
        return block, d, far

    def pass_on(t):
        block, d, far = where_is(t)

        def passed():
            with jax.named_scope("A_pass"):
                p_arrival(d, far).wait_recv()
            t_copy(d, far, core).start()

        pl.when(far > 0)(passed)

    last = jnp.minimum(index, reach * plane)
    pl.when(last > 0)(lambda: pass_on(1))

    def step(t, carry):
        pl.when((t < last) & (t != place + 1))(lambda: pass_on(t + 1))
        block, d, far = where_is(t)
        with jax.named_scope("A_wait"):
            t_copy(d, far, 1 - core).wait_recv()
        with jax.named_scope("A_block"):
            attend(block, False)

        @pl.when(t == place + 1)
        def _():
            for d in range(2, reach + 1):
                relay(d)
            pl.when(t < last)(lambda: pass_on(t + 1))

        return carry

    lax.fori_loop(1, last + 1, step, 0)

    for h in range(heads):
        done = (acc[h] / total[h : h + 1, :]).astype(jnp.bfloat16)
        for part in range(2):
            halves[part, h * VALUE_ENTRIES : (h + 1) * VALUE_ENTRIES, :] = done[:, part * half : (part + 1) * half]
    swap = remote(halves.at[1 - core], full.at[core], x_send, x_recv, (index, 1 - core))
    swap.start()
    full[core] = halves[core]
    loads[10].wait()
    loads[11].wait()
    with jax.named_scope("A_swap"):
        remote(halves.at[core], full.at[1 - core], x_send, x_recv, (index, 1 - core)).wait_recv()
    width = proj.shape[1]
    tile = math.gcd(width, 512)
    attended = full[...].reshape(proj.shape[0], half).astype(jnp.float32).T.astype(jnp.bfloat16)

    def project(j, carry):
        columns = pl.ds(pl.multiple_of(j * tile, tile), tile)
        mix[:, columns] = jnp.dot(attended, proj[:, columns], preferred_element_type=jnp.float32)
        return carry

    with jax.named_scope("A_project"):
        lax.fori_loop(0, width // tile, project, 0)

    def settle(j, carry):
        some = pl.ds(pl.multiple_of(j * 16, 16), 16)
        branch = rms_scale(mix[some, :], mix_gain[...])
        kept = (residual[some, :].astype(jnp.float32) + branch).astype(jnp.bfloat16)
        middle[some, :] = kept
        normed[some, :] = rms_scale(kept.astype(jnp.float32), moe_gain[...]).astype(jnp.bfloat16)
        return carry

    with jax.named_scope("A_settle"):
        lax.fori_loop(0, half // 16, settle, 0, unroll=2)
    group_rows = grouped.shape[1]
    slots = groups * group_rows
    chooser[...] = jnp.where(
        lax.broadcasted_iota(jnp.int32, (slots, half), 0).astype(jnp.float32) == member, 1.0, 0.0
    ).astype(jnp.bfloat16)

    def ready(group):
        picks = chooser[pl.ds(pl.multiple_of(group * group_rows, group_rows), group_rows), :]
        for j in range(width // tile):
            columns = slice(j * tile, (j + 1) * tile)
            grouped[group, :, columns] = jnp.dot(
                picks, normed[:, columns], preferred_element_type=jnp.float32
            ).astype(jnp.bfloat16)

    spots[...] = chooser[...].astype(jnp.float32).T.astype(jnp.bfloat16)
    cut = width // PARTS

    def out_copy(part):
        columns = slice(part * cut, (part + 1) * cut)
        return pltpu.make_async_copy(total_out.at[part], out_ref.at[:, columns], o_sem.at[part])

    def conclude(part):
        columns = slice(part * cut, (part + 1) * cut)
        blended = jnp.dot(
            spots[...], returned[:, :, columns].reshape(slots, cut), preferred_element_type=jnp.float32
        )
        total_out[part] = (middle[:, columns].astype(jnp.float32) + blended).astype(jnp.bfloat16)
        out_copy(part).start()

    def settle_sends():
        swap.wait_send()
        for d in range(reach + 1):
            for far in range(0 if d else 1, plane):
                pl.when((level >= d) if far == 0 else wanted(d, far, False))(
                    lambda d=d, far=far: t_copy(d, far, core).wait_send()
                )
                if far:
                    pl.when(wanted(d, far, True))(lambda d=d, far=far: p_copy(d, far).wait_send())
        for d in range(1, reach + 1):
            pl.when(level + d < groups)(lambda d=d: z_copy(d).wait_send())
        for k in range(1, groups):
            m_copy(k).wait_send()

    for copy in loads[12:]:
        copy.wait()
    expert_stage(
        groups, plane, (index, core, level, place), ready, settle_sends, conclude, grouped, metas, returned,
        gate, up, down, *rest[:9], m_send, m_recv, *rest[9:],
    )

    for part in range(PARTS):
        out_copy(part).wait()


def layer(
    queries, latent, rope_key, wk, wv, proj, residual, expert_ids, doc_ids, route,
    mix_gain, moe_gain, gate, up, down, count,
):
    rows, rank = latent.shape
    half = rows // 2
    plane = count // GROUPS
    capacity = half // plane
    heads = wk.shape[1] // UNROTATED_DIM
    width = proj.shape[1]
    units = gate.shape[1]
    group_rows = half // 2
    cut = width // PARTS
    hbm = pl.BlockSpec(memory_space=pltpu.HBM)
    dma = pltpu.SemaphoreType.DMA
    few, many = dma((GROUPS,)), dma((GROUPS * plane,))
    few_parts, many_parts = dma((GROUPS * PARTS,)), dma((GROUPS * PARTS * plane,))

    def held(*shape, dtype=jnp.bfloat16):
        return pltpu.VMEM(shape, dtype)

    loaded = (
        queries.T, latent, rope_key.T, wk, wv, proj, residual, expert_ids.T, doc_ids[None, :],
        route.T, mix_gain[None, :], moe_gain[None, :], gate, up, down,
    )
    table = held(GROUPS, 16, -(-group_rows // 128) * 128)
    block = held(GROUPS, PARTS, plane, capacity, cut)
    return pl.pallas_call(
        functools.partial(layer_kernel, GROUPS, plane, heads),
        out_shape=jax.ShapeDtypeStruct((half, width), jnp.bfloat16),
        in_specs=[hbm] * len(loaded),
        out_specs=hbm,
        scratch_shapes=[held(*array.shape, dtype=array.dtype) for array in loaded] + [
            held(half, width), held(GROUPS * group_rows, half), held(GROUPS, group_rows, width),
            held(half, GROUPS * group_rows), held(PARTS, half, cut),
            held(count, 2, half + ROPE, rank),
            held(heads, HEAD_LANES, rows),
            held(heads * VALUE_ENTRIES, rank),
            held(heads, rows, dtype=jnp.float32),
            held(heads, rows, dtype=jnp.float32),
            held(heads, VALUE_ENTRIES, rows, dtype=jnp.float32),
            held(2, heads * VALUE_ENTRIES, half),
            held(2, heads * VALUE_ENTRIES, half),
            held(half, width, dtype=jnp.float32),
            held(half, width),
            held(GROUPS, group_rows, width), table, table,
            dma((len(loaded),)), dma((PARTS,)), few, few, many, many, many, many, dma, dma, few, few,
            held(GROUPS, group_rows, width),
            held(GROUPS, plane, capacity, width),
            held(GROUPS, 2, plane, capacity, width),
            held(2 * plane * capacity, units),
            held(GROUPS, PARTS, 2, plane, capacity, cut),
            block, block, block,
            held(GROUPS, PARTS, group_rows, cut),
            few, few, many, many, few, many, many,
            few_parts, few_parts, many_parts, many_parts, few_parts, few_parts, few_parts,
        ],
        compiler_params=pltpu.CompilerParams(
            collective_id=3, has_side_effects=True, vmem_limit_bytes=VMEM_GRANT
        ),
        name="layer",
    )(*loaded)


def local(
    residual,
    queries,
    latent,
    rope_key,
    doc_ids,
    latent_to_key,
    latent_to_value,
    out_proj,
    mix_gain,
    moe_gain,
    expert_ids,
    route_weight,
    gate_weight,
    up_weight,
    down_weight,
):
    return layer(
        queries, latent, rope_key, latent_to_key, latent_to_value, out_proj, residual,
        expert_ids, doc_ids, route_weight, mix_gain, moe_gain, gate_weight[0], up_weight[0],
        down_weight[0], lax.axis_size("sp"),
    )


def solution(mesh):
    in_specs = (
        P(("sp", "tp"), None),
        P("sp", "tp"),
        P("sp", None),
        P("sp", None),
        P("sp"),
        P(None, "tp"),
        P(None, "tp"),
        P(),
        P(),
        P(),
        P(("sp", "tp"), None),
        P(("sp", "tp"), None),
        P("sp", None, "tp"),
        P("sp", None, "tp"),
        P("sp", "tp", None),
    )
    out_specs = P(("sp", "tp"), None)
    return jax.shard_map(local, mesh=mesh, in_specs=in_specs, out_specs=out_specs, check_vma=False)
```
